32 devices in a mesh: sp: 16 (over z, y, core), tp: 2 (over x).
Axes of the slice: x: 2, y: 2, z: 4, core: 2. Of those that a mesh axis runs over, the one named last changes fastest.
Arguments:
- stream: bfloat16 [16384, 2048], P('sp'), may hold values from -6 to 6
- queries: bfloat16 [16384, 1024], P('sp', 'tp'), may hold values from -6 to 6
- projected_keys: bfloat16 [16384, 1024], P('sp', 'tp'), may hold values from -6 to 6
- values: bfloat16 [16384, 2048], P('sp', 'tp'), may hold values from -6 to 6
- decay_gate_logits: bfloat16 [16384, 1024], P('sp', 'tp'), may hold values from -7 to 7
- decay_gate_bias: float32 [1024], P('tp')
- extra_log_decay: float32 [16384, 8], P('sp', 'tp'), may hold values from -0.7 to 0
- document_index: int32 [16384], P('sp'), may hold values from 0 to 3, never falling along the last dimension, each value on 1 to 8192 neighbouring positions
- output_gate: bfloat16 [16384, 2048], P('sp', 'tp'), may hold values from -6 to 6
- head_norm_gain: bfloat16 [256], replicated, may hold values from 0.099609375 to 1.8984375
- output_weight: bfloat16 [2048, 2048], P('tp'), may hold values from -0.125 to 0.125
- feedforward_norm_gain: bfloat16 [2048], replicated, may hold values from 0.099609375 to 1.8984375
- gate_weight: bfloat16 [2048, 5632], P('sp', 'tp'), may hold values from -0.125 to 0.125
- up_weight: bfloat16 [2048, 5632], P('sp', 'tp'), may hold values from -0.125 to 0.125
- down_weight: bfloat16 [5632, 2048], P('tp', 'sp'), may hold values from -0.078125 to 0.078125
Outputs:
- updated: bfloat16 [16384, 2048], P(('sp', 'tp'))
The draws below stay inside these ranges and needn't reach their ends.
All inputs are finite; a program needn't handle non-finite values.
Results may differ from the reference program's by a relative error of at most 0.015.
Values may be sent and summed in bfloat16 or wider, within the bound.
A program may use at most 128 MiB of HBM per device.

```python
import math
import jax
import jax.numpy as jnp
import numpy as np
from jax import lax

D = 2048
FF = 5632
HEAD_TOTAL = 8
DK = 128
DV = 256
BLOCK_LENGTH = 64
TOK_DEV = 1024
TOKENS = 16384
QK = 1024
VDIM = 2048
N_SP = 16
N_TP = 2


def draw_decay_gate_logits(key, part):
    noise_key, shift_key = jax.random.split(jax.random.fold_in(key, 11))
    blocks = TOKENS // TOK_DEV
    block_shift = jax.random.uniform(shift_key, (blocks, 1, 1), jnp.float32, -0.7, 0.7)
    noise_part = jnp.clip(jax.random.normal(noise_key, (blocks, TOK_DEV, QK), jnp.float32), -6.0, 6.0)
    return (noise_part + block_shift).reshape(TOKENS, QK).astype(jnp.bfloat16)


def draw_decay_gate_bias(key, part):
    slow_key, fast_key, level_key = jax.random.split(jax.random.fold_in(key, 23), 3)
    slow_heads = jax.random.uniform(slow_key, (HEAD_TOTAL,), jnp.float32) < 0.5
    base_level = jnp.log(jnp.float32(TOKENS)) - 2.0
    slow_level = base_level + jax.random.uniform(level_key, (HEAD_TOTAL, DK), jnp.float32, 0.0, 2.0)
    fast_level = jax.random.uniform(fast_key, (HEAD_TOTAL, DK), jnp.float32, 0.0, 1.0)
    return jnp.where(slow_heads[:, None], slow_level, fast_level).reshape(HEAD_TOTAL * DK)


def draw_extra_log_decay(key, part):
    place_key, size_random_key = jax.random.split(jax.random.fold_in(key, 37))
    head_keys = jax.random.split(place_key, HEAD_TOTAL)
    orders = jax.vmap(lambda single: jax.random.permutation(single, TOKENS))(head_keys)
    places = jnp.transpose(orders[:, :3])
    extra_decay_sizes = jnp.log(jax.random.uniform(size_random_key, (3, HEAD_TOTAL), jnp.float32, 0.5, 0.8))
    positions = jnp.arange(TOKENS)[:, None, None]
    matched_positions = (positions == places[None]).astype(jnp.float32)
    return jnp.sum(matched_positions * extra_decay_sizes[None], axis=1)


def steps_of(stream_key, dims, cuts, smallest, high):
    def one(dim, blocks):
        draws = jax.random.uniform(jax.random.fold_in(jax.random.fold_in(stream_key, 6), dim), (blocks,), jnp.float32, smallest / len(cuts), high / len(cuts))
        return jnp.repeat(jnp.exp(draws), dims[dim] // blocks).reshape((-1,) + (1,) * (len(dims) - dim - 1))

    level = one(*cuts[0])
    for cut in cuts[1:]:
        level = level * one(*cut)
    return level


def split_up(number_of, total, reach, slope):
    loads = [(1 << 20) // math.isqrt(rank ** slope) + 1 for rank in range(2, number_of + 1)]
    spare, given = total - reach - (number_of - 1), [1] * (number_of - 1)
    while spare > 0:
        free = [i for i in range(number_of - 1) if given[i] < reach]
        whole, budget = sum([loads[i] for i in free]), spare
        for i in free:
            addition = min(reach - given[i], max(1, budget * loads[i] // whole), spare)
            given[i] = given[i] + addition
            spare = spare - addition
    return np.array([reach] + given)


def uneven_parts(stream_key, number_of, total, most, skew):
    if number_of == 2:
        one = jax.random.randint(stream_key, (), max(1, total - most), min(most, total - 1) + 1)
        return jnp.stack([one, total - one])
    lengths = jnp.asarray(split_up(number_of, total, most, skew), jnp.int32)
    couples = (number_of - 1) // 2
    giver, receiver = lengths[1:1 + 2 * couples:2], lengths[2:2 + 2 * couples:2]
    margin = jnp.minimum(giver - 1, most - receiver)
    passed = jax.random.randint(jax.random.fold_in(stream_key, 1), (couples,), 0, 1 << 20) % (margin + 1)
    lengths = lengths.at[1:1 + 2 * couples:2].set(giver - passed).at[2:2 + 2 * couples:2].set(receiver + passed)
    return lengths[jax.random.permutation(jax.random.fold_in(stream_key, 2), number_of)]


def gaussian(rng, dims, spread, reach, shards=(), kind=jnp.bfloat16):
    values = jax.random.normal(rng, dims, jnp.float32) * spread
    if len(shards) > 0:
        values = steps_of(rng, dims, shards, -0.22, 0.18) * values
    return jnp.clip(values, min=-reach, max=reach).astype(kind)


def setup_inputs(seed: int = 0) -> dict:
    splits = jax.random.split(jax.random.key(seed), 16)
    stream = gaussian(splits[0], (TOKENS, D), 1.0, 6.0, ((0, 16),))
    queries = gaussian(splits[1], (TOKENS, QK), 1.0, 6.0, ((0, 16), (1, 2)))
    projected_keys = gaussian(splits[2], (TOKENS, QK), 1.0, 6.0, ((0, 16), (1, 2)))
    values = gaussian(splits[3], (TOKENS, VDIM), 1.0, 6.0, ((0, 16), (1, 2)))
    decay_gate_logits = draw_decay_gate_logits(jax.random.fold_in(splits[15], 71), 0)
    decay_gate_bias = draw_decay_gate_bias(jax.random.fold_in(splits[15], 71), 0)
    extra_log_decay = draw_extra_log_decay(jax.random.fold_in(splits[15], 71), 0)
    document_index = jnp.searchsorted(jnp.cumsum(uneven_parts(splits[7], N_SP // 4, TOKENS, TOKENS // 2, 0)), jnp.arange(TOKENS), side="right").astype(jnp.int32)
    output_gate = gaussian(splits[8], (TOKENS, VDIM), 1.0, 6.0, ((0, 16), (1, 2)))
    head_norm_gain = jnp.clip(1.0 + 0.18 * jax.random.normal(splits[9], (DV,), jnp.float32), 0.099609375, 1.8984375).astype(jnp.bfloat16)
    output_weight = gaussian(splits[10], (VDIM, D), VDIM ** -0.5, 0.125, ((0, 2),))
    feedforward_norm_gain = jnp.clip(1.0 + 0.18 * jax.random.normal(splits[11], (D,), jnp.float32), 0.099609375, 1.8984375).astype(jnp.bfloat16)
    gate_weight = gaussian(splits[12], (D, FF), D ** -0.5, 0.125, ((0, 16), (1, 2)))
    up_weight = gaussian(splits[13], (D, FF), D ** -0.5, 0.125, ((0, 16), (1, 2)))
    down_weight = gaussian(splits[14], (FF, D), FF ** -0.5, 0.078125, ((0, 2), (1, 16)))
    return {"stream": stream, "queries": queries, "projected_keys": projected_keys, "values": values, "decay_gate_logits": decay_gate_logits, "decay_gate_bias": decay_gate_bias, "extra_log_decay": extra_log_decay, "document_index": document_index, "output_gate": output_gate, "head_norm_gain": head_norm_gain, "output_weight": output_weight, "feedforward_norm_gain": feedforward_norm_gain, "gate_weight": gate_weight, "up_weight": up_weight, "down_weight": down_weight}


TAU = 16.0
EPS = 1e-06
HIGH = lax.Precision.HIGHEST

def combine(earlier, later):
    decay_e, state_e, entry_e, exit_e = earlier
    decay_l, state_l, entry_l, exit_l = later
    joined = (exit_e == entry_l) | (exit_e < 0.0) | (entry_l < 0.0)
    passing = decay_l * joined.astype(decay_l.dtype)[..., None, None]
    merged_state = state_l + passing[..., None] * state_e
    merged_decay = decay_e * passing
    entry_doc = jnp.where(entry_e < 0.0, entry_l, entry_e)
    exit_doc = jnp.where(exit_l < 0.0, exit_e, exit_l)
    return (merged_decay, merged_state, entry_doc, exit_doc)

def neutral(head_number, key_channels, val_dim):
    return (jnp.ones((head_number, key_channels), jnp.float32), jnp.zeros((head_number, key_channels, val_dim), jnp.float32), jnp.full((), -1.0, jnp.float32), jnp.full((), -1.0, jnp.float32))

def block_prefix(elements, initial, reverse_dir):

    def advance(running, element):
        return (combine(running, element), running)
    totals, before = lax.scan(advance, initial, elements, reverse=reverse_dir)
    return (before, totals)

def attention_variant(queries, projected_keys, values, decay_gate_logits, decay_gate_bias, extra_log_decay, document_index, block_length):
    head_number = extra_log_decay.shape[1]
    row_number = queries.shape[0]
    blocks = row_number // block_length
    key_channels = queries.shape[1] // head_number
    val_dim = values.shape[1] // head_number
    query_f = queries.astype(jnp.float32).reshape(blocks, block_length, head_number, key_channels) * key_channels ** (-0.5)
    key_f = projected_keys.astype(jnp.float32).reshape(blocks, block_length, head_number, key_channels)
    value_b = values.reshape(blocks, block_length, head_number, val_dim)
    decay_logarithm = jax.nn.log_sigmoid(decay_gate_logits.astype(jnp.float32) + decay_gate_bias) / TAU
    decay_logarithm = decay_logarithm.reshape(row_number, head_number, key_channels) + extra_log_decay[:, :, None]
    cumulative = jnp.cumsum(decay_logarithm.reshape(blocks, block_length, head_number, key_channels), axis=1)
    document_float = document_index.astype(jnp.float32).reshape(blocks, block_length)
    middle = cumulative[:, block_length // 2 - 1:block_length // 2]
    rising = jnp.exp(cumulative - middle)
    falling = jnp.exp(middle - cumulative)
    forward = jnp.einsum('bihc,bjhc->bhij', (query_f * rising).astype(jnp.bfloat16), (key_f * falling).astype(jnp.bfloat16), preferred_element_type=jnp.float32)
    backward = jnp.einsum('bihc,bjhc->bhij', (query_f * falling).astype(jnp.bfloat16), (key_f * rising).astype(jnp.bfloat16), preferred_element_type=jnp.float32)
    offsets = jnp.arange(block_length)
    same_doc = (document_float[:, :, None] == document_float[:, None, :])[:, None]
    below_mask = offsets[None, :] <= offsets[:, None]
    above_mask = offsets[None, :] >= offsets[:, None]
    scores = jnp.where(same_doc & below_mask, forward, 0.0) + jnp.where(same_doc & above_mask, backward, 0.0)
    within_block = jnp.einsum('bhij,bjhv->bihv', scores.astype(jnp.bfloat16), value_b, preferred_element_type=jnp.float32)
    block_end = cumulative[:, block_length - 1]
    first_doc = document_float[:, 0]
    last_doc = document_float[:, block_length - 1]
    through = jnp.exp(block_end) * (first_doc == last_doc).astype(jnp.float32)[:, None, None]
    tail_mask = (document_float == last_doc[:, None]).astype(jnp.float32)[:, :, None, None]
    head_mask = (document_float == first_doc[:, None]).astype(jnp.float32)[:, :, None, None]
    tail_keys = (key_f * jnp.exp(block_end[:, None] - cumulative) * tail_mask).astype(jnp.bfloat16)
    head_keys = (key_f * jnp.exp(cumulative) * head_mask).astype(jnp.bfloat16)
    fwd_state = jnp.einsum('bjhc,bjhv->bhcv', tail_keys, value_b, preferred_element_type=jnp.float32)
    bwd_state = jnp.einsum('bjhc,bjhv->bhcv', head_keys, value_b, preferred_element_type=jnp.float32)
    forward_elements = (through, fwd_state, first_doc, last_doc)
    backward_elements = (through, bwd_state, last_doc, first_doc)
    forward_query = query_f * jnp.exp(cumulative)
    backward_query = query_f * jnp.exp(block_end[:, None] - cumulative)
    return (within_block, forward_elements, backward_elements, forward_query, backward_query, document_float)

def carried(inflow, factor, document_float):
    hit_mask = (document_float == inflow[3][:, None]).astype(jnp.float32)[:, :, None, None]
    return jnp.einsum('bihc,bhcv->bihv', factor, inflow[1], precision=HIGH) * hit_mask

def head_mix(within_block, fwd_in, bwd_in, forward_query, backward_query, document_float, output_gate, head_norm_gain, head_number):
    total_out = within_block + carried(fwd_in, forward_query, document_float) + carried(bwd_in, backward_query, document_float)
    row_number = output_gate.shape[0]
    total_out = total_out.reshape(row_number, head_number, -1)
    scaled = total_out * lax.rsqrt(lax.optimization_barrier(jnp.mean(total_out * total_out, axis=-1, keepdims=True)) + EPS)
    scaled = scaled * head_norm_gain.astype(jnp.float32)
    return (scaled.reshape(row_number, -1) * jax.nn.silu(output_gate.astype(jnp.float32))).astype(jnp.bfloat16)

def row_norm(rows_f, gain):
    factor = lax.rsqrt(lax.optimization_barrier(jnp.mean(rows_f * rows_f, axis=-1, keepdims=True)) + EPS)
    return (rows_f * factor * gain.astype(jnp.float32)).astype(jnp.bfloat16)

def reference(stream, queries, projected_keys, values, decay_gate_logits, decay_gate_bias, extra_log_decay, document_index, output_gate, head_norm_gain, output_weight, feedforward_norm_gain, gate_weight, up_weight, down_weight):
    head_number = extra_log_decay.shape[1]
    key_channels = queries.shape[1] // head_number
    val_dim = values.shape[1] // head_number
    within_block, forward_elements, backward_elements, forward_query, backward_query, document_float = attention_variant(queries, projected_keys, values, decay_gate_logits, decay_gate_bias, extra_log_decay, document_index, BLOCK_LENGTH)
    initial = neutral(head_number, key_channels, val_dim)
    fwd_in = block_prefix(forward_elements, initial, False)[0]
    bwd_in = block_prefix(backward_elements, initial, True)[0]
    head_mixed = head_mix(within_block, fwd_in, bwd_in, forward_query, backward_query, document_float, output_gate, head_norm_gain, head_number)
    col_group = values.shape[1] // N_TP
    attended = jnp.zeros(stream.shape, jnp.float32)
    for group_idx in range(N_TP):
        lower_col = group_idx * col_group
        partial_value = jnp.dot(head_mixed[:, lower_col:lower_col + col_group], output_weight[lower_col:lower_col + col_group], preferred_element_type=jnp.float32)
        attended = attended + lax.optimization_barrier(partial_value.astype(jnp.bfloat16)).astype(jnp.float32)
    resid = stream.astype(jnp.float32) + attended
    normed = row_norm(resid, feedforward_norm_gain)
    unit_group = gate_weight.shape[1] // N_TP
    mlp_out = jnp.zeros(stream.shape, jnp.float32)
    for group_idx in range(N_TP):
        lower_unit = group_idx * unit_group
        gate_act = jnp.dot(normed, gate_weight[:, lower_unit:lower_unit + unit_group], preferred_element_type=jnp.float32)
        up_act = jnp.dot(normed, up_weight[:, lower_unit:lower_unit + unit_group], preferred_element_type=jnp.float32)
        hidden = (jax.nn.silu(gate_act) * up_act).astype(jnp.bfloat16)
        partial_value = jnp.dot(hidden, down_weight[lower_unit:lower_unit + unit_group], preferred_element_type=jnp.float32)
        mlp_out = mlp_out + lax.optimization_barrier(partial_value.astype(jnp.bfloat16)).astype(jnp.float32)
    return (resid + mlp_out).astype(jnp.bfloat16)
```

```python
import functools

import jax
import jax.numpy as jnp
from jax import lax
from jax.experimental import pallas as pl
from jax.experimental.pallas import tpu as pltpu
from jax.sharding import PartitionSpec as P

BLOCK_LENGTH = 64
TAU = 16.0
EPS = 1e-06
HIGH = lax.Precision.HIGHEST
NT = (((1,), (1,)), ((), ()))
TN = (((0,), (0,)), ((), ()))


def shard_states(blocks, size, k_ref, v_ref, decay_ref, doc_ref, cum_ref, state_ref, log_ref,
                 tail_ref, lead_ref):
    rows = lax.broadcasted_iota(jnp.int32, (size, size), 0)
    cols = lax.broadcasted_iota(jnp.int32, (size, size), 1)
    lower = (cols <= rows).astype(jnp.float32)
    before = jnp.zeros((1, k_ref.shape[1]), jnp.float32)
    starts = []
    for b in range(blocks):
        here = pl.ds(b * size, size)
        cum = jnp.dot(lower, decay_ref[here, :], precision=HIGH,
                      preferred_element_type=jnp.float32)
        cum_ref[here, :] = cum
        starts.append(before)
        before = before + cum[size - 1 : size]
    total = before
    first = doc_ref[0:1, :]
    last = doc_ref[blocks * size - 1 : blocks * size, :]
    for b in range(blocks):
        here = pl.ds(b * size, size)
        cum = cum_ref[here, :] + starts[b]
        keys = k_ref[here, :].astype(jnp.float32)
        doc = doc_ref[here, :]
        tail_ref[here, :] = jnp.where(doc == last, keys * jnp.exp(total - cum), 0.0).astype(
            jnp.bfloat16)
        lead_ref[here, :] = jnp.where(doc == first, keys * jnp.exp(cum), 0.0).astype(
            jnp.bfloat16)
    values = v_ref[...]
    state_ref[0, 0] = lax.dot_general(
        tail_ref[...], values, TN, preferred_element_type=jnp.float32).astype(jnp.bfloat16)
    state_ref[1, 0] = lax.dot_general(
        lead_ref[...], values, TN, preferred_element_type=jnp.float32).astype(jnp.bfloat16)
    log_ref[0] = jnp.broadcast_to(total, log_ref.shape[1:])


def head_outputs(blocks, size, q_ref, k_ref, v_ref, cum_ref, doc_ref, same_ref, gate_ref,
                 gain_ref, carry_ref, out_ref, back_ref):
    scale = q_ref.shape[1] ** (-0.5)
    later = carry_ref[1, 0]
    for b in reversed(range(blocks)):
        here = pl.ds(b * size, size)
        back_ref[b] = later.astype(jnp.bfloat16)
        if b:
            cum = cum_ref[here, :]
            doc = doc_ref[here, :]
            first, last = doc[0:1], doc[size - 1 : size]
            previous = doc_ref[b * size - 1 : b * size, :]
            lead = jnp.where(doc == first, k_ref[here, :].astype(jnp.float32) * jnp.exp(cum), 0.0)
            added = lax.dot_general(lead.astype(jnp.bfloat16), v_ref[here, :], TN,
                                    preferred_element_type=jnp.float32)
            through = jnp.where(first == last, jnp.exp(cum[size - 1 : size]), 0.0)
            later = added + jnp.transpose(through) * later
            later = jnp.where(jnp.transpose(previous == first), later, 0.0)
    earlier = carry_ref[0, 0]
    rows = lax.broadcasted_iota(jnp.int32, (size, size), 0)
    cols = lax.broadcasted_iota(jnp.int32, (size, size), 1)
    for b in range(blocks):
        here = pl.ds(b * size, size)
        cum = cum_ref[here, :]
        doc = doc_ref[here, :]
        first, last = doc[0:1], doc[size - 1 : size]
        end = cum[size - 1 : size]
        query = q_ref[here, :].astype(jnp.float32) * scale
        keys = k_ref[here, :].astype(jnp.float32)
        values = v_ref[here, :]
        middle = cum[size // 2 - 1 : size // 2]
        rising = jnp.exp(cum - middle)
        falling = jnp.exp(middle - cum)
        forward = lax.dot_general((query * rising).astype(jnp.bfloat16),
                                  (keys * falling).astype(jnp.bfloat16), NT,
                                  preferred_element_type=jnp.float32)
        backward = lax.dot_general((query * falling).astype(jnp.bfloat16),
                                   (keys * rising).astype(jnp.bfloat16), NT,
                                   preferred_element_type=jnp.float32)
        same = same_ref[here, :] > 0.0
        scores = jnp.where(same & (cols <= rows), forward, 0.0) + jnp.where(
            same & (cols >= rows), backward, 0.0)
        total = jnp.dot(scores.astype(jnp.bfloat16), values, preferred_element_type=jnp.float32)
        shrink = jnp.exp(end - cum)
        onward = jnp.where(doc == first, query * jnp.exp(cum), 0.0).astype(jnp.bfloat16)
        rearward = jnp.where(doc == last, query * shrink, 0.0).astype(jnp.bfloat16)
        total = total + jnp.dot(onward, earlier.astype(jnp.bfloat16),
                                preferred_element_type=jnp.float32)
        total = total + jnp.dot(rearward, back_ref[b], preferred_element_type=jnp.float32)
        if b < blocks - 1:
            tail = jnp.where(doc == last, keys * shrink, 0.0)
            added = lax.dot_general(tail.astype(jnp.bfloat16), values, TN,
                                    preferred_element_type=jnp.float32)
            through = jnp.where(first == last, jnp.exp(end), 0.0)
            following = doc_ref[(b + 1) * size : (b + 1) * size + 1, :]
            earlier = added + jnp.transpose(through) * earlier
            earlier = jnp.where(jnp.transpose(last == following), earlier, 0.0)
        scaled = total * lax.rsqrt(jnp.mean(total * total, axis=-1, keepdims=True) + EPS)
        gate = gate_ref[here, :].astype(jnp.float32)
        scaled = scaled * gain_ref[...] * (gate / (1.0 + jnp.exp(-gate)))
        out_ref[here, :] = scaled.astype(jnp.bfloat16)


def row_norm(rows_f, gain):
    factor = lax.rsqrt(jnp.mean(rows_f * rows_f, axis=-1, keepdims=True) + EPS)
    return (rows_f * factor * gain.astype(jnp.float32)).astype(jnp.bfloat16)


def product(a, b):
    return jnp.dot(a, b, preferred_element_type=jnp.float32)


def carried_in(state, logs, leaves, enters, way):
    size = lax.axis_size("sp")
    me = lax.axis_index("sp")

    def from_away(distance, state, small):
        pairs = [(s, s + way * distance) for s in range(size) if 0 <= s + way * distance < size]
        return (lax.ppermute(state, "sp", pairs), lax.ppermute(small, "sp", pairs))

    def packed(logs, document):
        return jnp.concatenate([logs, jnp.full((1, logs.shape[1]), document)])

    state, small = from_away(1, state, packed(logs, leaves))
    place = me if way > 0 else size - 1 - me
    have = place >= 1
    state = jnp.where(have, state.astype(jnp.float32), 0.0)
    logs = jnp.where(have, small[:-1], 0.0)
    document = jnp.where(have, small[-1, 0], -1.0)
    distance = 1
    while distance < size - 1:
        far, small = from_away(distance, state.astype(jnp.bfloat16), packed(logs, document))
        reach = (place > distance) & (small[-1, 0] == document)
        weight = jnp.where(reach, jnp.exp(logs), 0.0)
        state = state + weight[..., None] * far.astype(jnp.float32)
        logs = logs + small[:-1]
        distance *= 2
    return jnp.where(document == enters, state, 0.0)


def attention(queries, projected_keys, values, decay_gate_logits, decay_gate_bias,
              extra_log_decay, document_index, output_gate, head_norm_gain, up_weight, gate_full):
    heads = extra_log_decay.shape[1]
    rows = queries.shape[0]
    dk = queries.shape[1] // heads
    dv = values.shape[1] // heads
    size = BLOCK_LENGTH
    blocks = rows // size
    decay = jax.nn.log_sigmoid(decay_gate_logits.astype(jnp.float32) + decay_gate_bias) / TAU
    decay = (decay.reshape(rows, heads, dk) + extra_log_decay[:, :, None]).reshape(rows, -1)
    doc = document_index.astype(jnp.float32)
    doc_wide = jnp.broadcast_to(doc[:, None], (rows, dk))
    by_block = doc.reshape(blocks, size)
    same = (by_block[:, :, None] == by_block[:, None, :]).astype(jnp.float32).reshape(rows, size)
    keyed = pl.BlockSpec((rows, dk), lambda h: (0, h))
    valued = pl.BlockSpec((rows, dv), lambda h: (0, h))
    fixed = pl.BlockSpec((rows, dk), lambda h: (0, 0))
    state_spec = pl.BlockSpec((2, 1, dk, dv), lambda h: (0, h, 0, 0))
    params = pltpu.CompilerParams(dimension_semantics=("arbitrary",),
                                  vmem_limit_bytes=40 * 1024 * 1024)
    cum, states, logs = pl.pallas_call(
        functools.partial(shard_states, blocks, size),
        grid=(heads,),
        out_shape=(
            jax.ShapeDtypeStruct((rows, heads * dk), jnp.float32),
            jax.ShapeDtypeStruct((2, heads, dk, dv), jnp.bfloat16),
            jax.ShapeDtypeStruct((heads, 8, dk), jnp.float32),
        ),
        in_specs=[keyed, valued, keyed, fixed],
        out_specs=(keyed, state_spec, pl.BlockSpec((1, 8, dk), lambda h: (h, 0, 0))),
        scratch_shapes=[pltpu.VMEM((rows, dk), jnp.bfloat16)] * 2,
        compiler_params=params,
        cost_estimate=pl.CostEstimate(flops=rows * heads * dk * dv * 4,
                                      bytes_accessed=rows * heads * dk * 20,
                                      transcendentals=rows * heads * dk * 2),
        name="shard_states",
    )(projected_keys, values, decay, doc_wide)
    first, last = doc[0], doc[rows - 1]
    logs = logs[:, 0]
    ahead = carried_in(states[0], logs, last, first, 1)
    ahead, up_weight, gate_full = lax.optimization_barrier((ahead, up_weight, gate_full))
    carry = jnp.stack([ahead, carried_in(states[1], logs, first, last, -1)])
    mixed = pl.pallas_call(
        functools.partial(head_outputs, blocks, size),
        grid=(heads,),
        out_shape=jax.ShapeDtypeStruct((rows, heads * dv), jnp.bfloat16),
        in_specs=[keyed, keyed, valued, keyed, fixed,
                  pl.BlockSpec((rows, size), lambda h: (0, 0)), valued,
                  pl.BlockSpec((1, dv), lambda h: (0, 0)), state_spec],
        out_specs=valued,
        scratch_shapes=[pltpu.VMEM((blocks, dk, dv), jnp.bfloat16)],
        compiler_params=params,
        cost_estimate=pl.CostEstimate(flops=rows * heads * dk * dv * 10,
                                      bytes_accessed=rows * heads * dk * 24,
                                      transcendentals=rows * heads * dk * 8),
        name="head_outputs",
    )(queries, projected_keys, values, cum, doc_wide, same, output_gate,
      head_norm_gain.astype(jnp.float32)[None], carry)
    return mixed, up_weight, gate_full


MESH = pl.DeviceIdType.MESH
Z1, Z2, Z3, YY, SS = 4, 8, 12, 2, 1
FIRST, LAST = 4, 5
WIDE = 256


class Net:
    def __init__(self, planes):
        place = lax.axis_index("sp")
        self.t = lax.axis_index("tp")
        self.c = place % 2
        self.y = (place // 2) % 2
        self.z = place // 4
        z = self.z
        self.zs = [z, z + 1 - 2 * (z % 2), (z + 2) % planes, planes - 1 - z]
        self.ys = [self.y, 1 - self.y]
        self.cs = [self.c, 1 - self.c]
        self.middle = (z == 1) | (z == 2)

    def chip(self, r):
        return self.zs[r // 4] * 2 + self.ys[(r // 2) % 2]

    def shard(self, r):
        return self.chip(r) * 2 + self.cs[r % 2]

    def dev(self, r):
        return (self.shard(r), self.t)

    def across(self):
        return (self.shard(0), 1 - self.t)


def maybe(cond, do):
    if cond is None:
        do()
    else:
        pl.when(cond)(do)


class Sends:
    def __init__(self):
        self.open = []

    def go(self, src, dst, send, recv, device, cond=None):
        copy = pltpu.make_async_remote_copy(src_ref=src, dst_ref=dst, send_sem=send, recv_sem=recv,
                                            device_id=device, device_id_type=MESH)
        maybe(cond, copy.start)
        self.open.append((copy, cond))

    def settle(self):
        copy, cond = self.open.pop()
        return functools.partial(maybe, cond, copy.wait_send)

    def drain(self):
        for copy, cond in self.open:
            maybe(cond, copy.wait_send)
        self.open = []


def arrived(ref, sem, cond=None):
    maybe(cond, pltpu.make_async_copy(ref, ref, sem).wait)


class Piece:
    def __init__(self, net, sends, own, full, recv, send, crossed):
        self.net, self.sends, self.own, self.full = net, sends, own, full
        self.recv, self.send, self.crossed, self.count = recv, send, crossed, 0

    def go(self, r, d, cond=None):
        dst = self.full(self.net.shard(r))
        self.sends.go(self.own if r == 0 else dst, dst, self.send.at[self.count],
                      self.recv.at[r ^ d], self.net.dev(d), cond)
        self.count += 1

    def wait(self, r):
        arrived(self.full(self.net.shard(r)), self.recv.at[r])

    def along(self, r):
        self.go(r, Z1)
        self.go(r, Z2)
        self.go(r, Z3, self.net.middle)

    def start_y(self):
        self.go(0, YY)

    def start_z(self):
        self.along(0)

    def start_s(self):
        self.go(0, SS)

    def start(self):
        self.start_y()
        self.start_z()
        self.start_s()

    def line(self, a):
        r = a * 4
        self.wait(r)
        if a == 2:
            self.go(r, Z1, self.net.middle)
        if not self.crossed:
            self.go(r, YY)
        self.go(r, SS)

    def beside(self, a):
        r = a * 4 + YY
        self.wait(r)
        if self.crossed:
            if a == 0:
                self.along(r)
            if a == 2:
                self.go(r, Z1, self.net.middle)
        self.go(r, SS)

    def near(self):
        for a in (1, 2):
            self.line(a)
            if self.crossed:
                self.beside(a)

    def far(self):
        self.line(3)
        if self.crossed:
            self.beside(3)

    def hand_over(self):
        for a in (0, 1, 2, 3):
            self.beside(a)

    def siblings(self):
        for a in range(4):
            for b in range(2):
                self.sibling(a, b)

    def sibling(self, a, b):
        self.wait(a * 4 + b * 2 + 1)


def column(rows, h):
    return jnp.transpose(rows)[:, h : h + 1]


def prefix_sums(blocks, size, h, decay, table):
    rows = lax.broadcasted_iota(jnp.int32, (size, size), 0)
    cols = lax.broadcasted_iota(jnp.int32, (size, size), 1)
    lower = (cols <= rows).astype(jnp.float32)
    total = jnp.zeros((1, decay.shape[2]), jnp.float32)
    for b in range(blocks):
        here = pl.ds(b * size, size)
        cum = jnp.dot(lower, decay[h, here, :], precision=HIGH, preferred_element_type=jnp.float32)
        decay[h, here, :] = cum
        total = total + cum[size - 1 : size]
    table[0, pl.ds(h, 1), :] = total


def own_states(blocks, size, h, q, k, v, cums, doc, table, onward, rearward, tail, lead, states):
    scale = q.shape[2] ** (-0.5)
    total = table[0, pl.ds(h, 1), :]
    first = doc[0:1, :]
    last = doc[blocks * size - 1 : blocks * size, :]
    before = jnp.zeros_like(total)
    for b in range(blocks):
        here = pl.ds(b * size, size)
        inner = cums[h, here, :]
        cum = inner + before
        before = before + inner[size - 1 : size]
        keys = k[h, here, :].astype(jnp.float32)
        query = q[h, here, :].astype(jnp.float32) * scale
        docs = doc[here, :]
        grown = jnp.where(docs == first, jnp.exp(cum), 0.0)
        shrunk = jnp.where(docs == last, jnp.exp(total - cum), 0.0)
        tail[here, :] = (keys * shrunk).astype(jnp.bfloat16)
        lead[here, :] = (keys * grown).astype(jnp.bfloat16)
        onward[h, here, :] = (query * grown).astype(jnp.bfloat16)
        rearward[h, here, :] = (query * shrunk).astype(jnp.bfloat16)
    values = v[h]
    states[0, h] = lax.dot_general(tail[...], values, TN,
                                   preferred_element_type=jnp.float32).astype(jnp.bfloat16)
    states[1, h] = lax.dot_general(lead[...], values, TN,
                                   preferred_element_type=jnp.float32).astype(jnp.bfloat16)


def inner_outputs(blocks, size, h, q, k, v, cums, doc, doc_row, back, out):
    scale = q.shape[2] ** (-0.5)
    rows = lax.broadcasted_iota(jnp.int32, (size, size), 0)
    cols = lax.broadcasted_iota(jnp.int32, (size, size), 1)
    later = jnp.zeros((k.shape[2], v.shape[2]), jnp.float32)
    for b in reversed(range(blocks)):
        here = pl.ds(b * size, size)
        back[b] = later.astype(jnp.bfloat16)
        if b:
            cum = cums[h, here, :]
            docs = doc[here, :]
            first, last = docs[0:1], docs[size - 1 : size]
            previous = doc[b * size - 1 : b * size, :]
            grown = jnp.where(docs == first, k[h, here, :].astype(jnp.float32) * jnp.exp(cum), 0.0)
            added = lax.dot_general(grown.astype(jnp.bfloat16), v[h, here, :], TN,
                                    preferred_element_type=jnp.float32)
            through = jnp.where(first == last, jnp.exp(cum[size - 1 : size]), 0.0)
            later = added + jnp.transpose(through) * later
            later = jnp.where(jnp.transpose(previous == first), later, 0.0)
    earlier = jnp.zeros((k.shape[2], v.shape[2]), jnp.float32)
    for b in range(blocks):
        here = pl.ds(b * size, size)
        cum = cums[h, here, :]
        docs = doc[here, :]
        first, last = docs[0:1], docs[size - 1 : size]
        end = cum[size - 1 : size]
        query = q[h, here, :].astype(jnp.float32) * scale
        keys = k[h, here, :].astype(jnp.float32)
        values = v[h, here, :]
        middle = cum[size // 2 - 1 : size // 2]
        rising = jnp.exp(cum - middle)
        falling = jnp.exp(middle - cum)
        forward = lax.dot_general((query * rising).astype(jnp.bfloat16),
                                  (keys * falling).astype(jnp.bfloat16), NT,
                                  preferred_element_type=jnp.float32)
        backward = lax.dot_general((query * falling).astype(jnp.bfloat16),
                                   (keys * rising).astype(jnp.bfloat16), NT,
                                   preferred_element_type=jnp.float32)
        same = docs[:, :size] == doc_row[b : b + 1, :]
        scores = jnp.where(same & (cols <= rows), forward, 0.0) + jnp.where(
            same & (cols >= rows), backward, 0.0)
        total = jnp.dot(scores.astype(jnp.bfloat16), values, preferred_element_type=jnp.float32)
        shrink = jnp.exp(end - cum)
        if b:
            onward = jnp.where(docs == first, query * jnp.exp(cum), 0.0).astype(jnp.bfloat16)
            total = total + jnp.dot(onward, earlier.astype(jnp.bfloat16),
                                    preferred_element_type=jnp.float32)
        if b < blocks - 1:
            rearward = jnp.where(docs == last, query * shrink, 0.0).astype(jnp.bfloat16)
            total = total + jnp.dot(rearward, back[b], preferred_element_type=jnp.float32)
            tail = jnp.where(docs == last, keys * shrink, 0.0)
            added = lax.dot_general(tail.astype(jnp.bfloat16), values, TN,
                                    preferred_element_type=jnp.float32)
            through = jnp.where(first == last, jnp.exp(end), 0.0)
            following = doc[(b + 1) * size : (b + 1) * size + 1, :]
            earlier = added + jnp.transpose(through) * earlier
            earlier = jnp.where(jnp.transpose(last == following), earlier, 0.0)
        out[h, here, :] = total


def finished_head(h, step, onward, rearward, inner, carry, gate, gain, mixed):
    def some(i, _):
        here = pl.ds(pl.multiple_of(i * step, step), step)
        total = inner[h, here, :]
        total = total + jnp.dot(onward[h, here, :], carry[0, h], preferred_element_type=jnp.float32)
        total = total + jnp.dot(rearward[h, here, :], carry[1, h],
                                preferred_element_type=jnp.float32)
        scaled = total * lax.rsqrt(jnp.mean(total * total, axis=-1, keepdims=True) + EPS)
        g = gate[h, here, :].astype(jnp.float32)
        mixed[h, here, :] = (scaled * gain[...] * (g / (1.0 + jnp.exp(-g)))).astype(jnp.bfloat16)
        return 0

    lax.fori_loop(0, inner.shape[1] // step, some, 0)


def layer_kernel(planes, size, pieces,
                 stream, queries, keys, values, decay, doc_wide, doc_row, out_gate, head_gain,
                 out_weight, norm_gain, gate_w, up_w, down_w,
                 result, gate_full, up_full, down_full,
                 q, k, v, cums, doc, og, onward, rearward, inner, tail, lead, back,
                 states, table, chip_state, plane_state, chip_carry, from_sib, from_y, from_z, carry,
                 mixed, mixed_x, weight, normed, resid, rows_in, hidden, narrow, part, part_x,
                 load_sem, own_sem, table_send, table_recv, state_send, state_recv,
                 piece_send, piece_recv, mix_send, mix_recv, wo_send, wo_recv, part_send, part_recv,
                 row_sem, wide_sem, narrow_sem, done_sem):
    net = Net(planes)
    sends = Sends()
    heads, rows, dk = q.shape
    dv = v.shape[2]
    blocks = rows // size
    c, y, z, t = net.c, net.y, net.z, net.t
    half = out_weight.shape[0]
    quarter = half // 2
    share = rows // 2

    loads = []
    for h in range(heads):
        group = []
        for n, (src, dst, width) in enumerate(((decay, cums, dk), (keys, k, dk), (queries, q, dk),
                                               (values, v, dv), (out_gate, og, dv))):
            group.append(pltpu.make_async_copy(src.at[:, h * width : (h + 1) * width], dst.at[h],
                                               load_sem.at[n, h]))
        loads.append(group)
    doc_load = pltpu.make_async_copy(doc_wide, doc, load_sem.at[5, 0])
    doc_load.start()
    for n in range(4):
        for h in range(heads):
            loads[h][n].start()
    for h in range(heads):
        loads[h][4].start()

    barrier = pltpu.get_barrier_semaphore()
    for r in range(1, 4 * planes):
        pl.semaphore_signal(barrier, inc=1, device_id=net.dev(r), device_id_type=MESH)
    pl.semaphore_signal(barrier, inc=1, device_id=net.across(), device_id_type=MESH)
    pl.semaphore_wait(barrier, 4 * planes)

    shards = {"g": (gate_w, gate_full), "u": (up_w, up_full), "d": (down_w, down_full)}

    def place(full, low, high, shard):
        if len(full.shape) == 3:
            return full.at[shard, low:high]
        own = full.shape[0] // (4 * planes)
        return full.at[pl.ds(pl.multiple_of(shard * own, own), own), low:high]

    ps = []
    for i, (name, low, high, crossed) in enumerate(pieces):
        own, full = shards[name]
        mine = own.at[low:high] if len(full.shape) == 3 else own.at[:, low:high]
        ps.append(Piece(net, sends, mine, functools.partial(place, full, low, high),
                        piece_recv.at[i], piece_send.at[i], crossed))
    gate_a_columns = pieces[0][2]
    gate_a, up_a, gate_b, up_b, down_a, down_b, cross_a, cross_b = ps
    gate_a.start()
    mine_low = pl.multiple_of(t * half, half)
    away_low = pl.multiple_of((1 - t) * half, half)
    sends.go(out_weight.at[pl.ds(pl.multiple_of(c * quarter, quarter), quarter)],
             weight.at[pl.ds(pl.multiple_of(t * half + c * quarter, quarter), quarter)],
             wo_send.at[0], wo_recv.at[0], net.across())
    own_copies = [pltpu.make_async_copy(out_weight, weight.at[pl.ds(mine_low, half)], own_sem.at[0])]
    me = net.shard(0)
    for i, (own, full) in enumerate(shards.values()):
        own_copies.append(pltpu.make_async_copy(
            own, place(full, 0, own.shape[len(full.shape) == 2], me), own_sem.at[i + 1]))

    for h in range(heads):
        loads[h][0].wait()
    doc_load.wait()
    table[0] = jnp.where(
        lax.broadcasted_iota(jnp.int32, table.shape[1:], 0) == FIRST,
        jnp.broadcast_to(doc[0:1, :], table.shape[1:]),
        jnp.broadcast_to(doc[rows - 1 : rows, :], table.shape[1:]))

    def sums(h, _):
        prefix_sums(blocks, size, h, cums, table)
        return 0

    lax.fori_loop(0, heads, sums, 0)
    for h in range(heads):
        for n in (1, 2, 3):
            loads[h][n].wait()

    def state_of(h, _):
        own_states(blocks, size, h, q, k, v, cums, doc, table, onward, rearward, tail, lead, states)
        return 0

    lax.fori_loop(0, 1, state_of, 0)
    for r in range(1, 4 * planes):
        sends.go(table.at[0], table.at[r], table_send.at[r], table_recv.at[r], net.dev(r))
    lax.fori_loop(1, heads, state_of, 0)
    sends.go(states.at[c], from_sib, state_send.at[0], state_recv.at[0], net.dev(SS))
    for copy in own_copies:
        copy.start()

    def state(r):
        return table[r]

    rising = c == 1

    def leaves(r):
        return jnp.where(rising, state(r)[LAST : LAST + 1], state(r)[FIRST : FIRST + 1])

    def enters(r):
        return jnp.where(rising, state(r)[FIRST : FIRST + 1], state(r)[LAST : LAST + 1])

    def chip_log(r):
        return state(r) + state(r ^ 1)

    def plane_log(a):
        return chip_log(a * 4) + chip_log(a * 4 + 2)

    arrived(table.at[1], table_recv.at[1])
    arrived(from_sib, state_recv.at[0])
    fade = jnp.where(leaves(1) == leaves(0), jnp.exp(state(0)), 0.0)
    way = 1 - c
    for h in range(heads):
        chip_state[h] = (states[way, h].astype(jnp.float32)
                         + column(fade, h) * from_sib[h].astype(jnp.float32)).astype(jnp.bfloat16)
    sends.go(chip_state, from_y, state_send.at[1], state_recv.at[1], net.dev(YY))

    def inner_of(h, _):
        inner_outputs(blocks, size, h, q, k, v, cums, doc, doc_row, back, inner)
        return 0

    lax.fori_loop(0, 2, inner_of, 0)
    for r in range(2, 4 * planes):
        arrived(table.at[r], table_recv.at[r])
    arrived(from_y, state_recv.at[1])
    upper = y == c
    fade = jnp.where(leaves(2) == leaves(0),
                     jnp.exp(jnp.where(upper, chip_log(0), chip_log(2))), 0.0)
    for h in range(heads):
        mine = chip_state[h].astype(jnp.float32)
        other = from_y[h].astype(jnp.float32)
        high = jnp.where(upper, mine, other)
        low = jnp.where(upper, other, mine)
        plane_state[h] = (high + column(fade, h) * low).astype(jnp.bfloat16)
    early, late = [None], [None]
    for a in range(1, planes):
        below = net.zs[a] < z
        early.append((rising & below) | ((c == 0) & (net.zs[a] > z)))
        late.append((rising & (net.zs[a] > z)) | ((c == 0) & below))
    for a in range(1, planes):
        sends.go(plane_state, from_z.at[a - 1], state_send.at[1 + a], state_recv.at[1 + a],
                 net.dev(a * 4), late[a])
    up_a.start_y()
    up_a.start_s()
    lax.fori_loop(2, heads, inner_of, 0)
    up_a.start_z()
    gate_a.near()
    for a in range(1, planes):
        arrived(from_z.at[a - 1], state_recv.at[1 + a], early[a])
    entry = enters(1)
    fades = []
    for a in range(1, planes):
        log = jnp.where(upper, chip_log(2), 0.0)
        for b in range(1, planes):
            if b != a:
                between = (net.zs[b] - net.zs[a]) * (z - net.zs[b]) > 0
                log = log + jnp.where(between, plane_log(b), 0.0)
        out_doc = jnp.where(upper, leaves(a * 4), leaves(a * 4 + 2))
        fades.append(jnp.where((out_doc == entry) & early[a], jnp.exp(log), 0.0))
    joins = jnp.where((leaves(2) == entry) & upper, jnp.ones_like(entry), 0.0)
    joins = jnp.broadcast_to(joins, (8, dk))
    through = jnp.where(enters(1) == leaves(1), jnp.exp(state(1)), 0.0)
    joined = jnp.broadcast_to(jnp.where(leaves(1) == enters(0), jnp.ones_like(entry), 0.0), (8, dk))
    for h in range(heads):
        into = column(joins, h) * from_y[h].astype(jnp.float32)
        for a in range(1, planes):
            into = into + column(fades[a - 1], h) * jnp.where(
                early[a], from_z[a - 1, h].astype(jnp.float32), 0.0)
        chip_carry[h] = into.astype(jnp.bfloat16)
        carry[way, h] = (column(joined, h) * (from_sib[h].astype(jnp.float32)
                                              + column(through, h) * into)).astype(jnp.bfloat16)
    sends.go(chip_carry, carry.at[way], state_send.at[5], state_recv.at[5], net.dev(SS))
    own_part = weight.at[pl.ds(pl.multiple_of((1 - t) * half + c * quarter, quarter), quarter)]
    sib_part = weight.at[pl.ds(pl.multiple_of((1 - t) * half + (1 - c) * quarter, quarter), quarter)]
    arrived(own_part, wo_recv.at[0])
    sends.go(own_part, own_part, wo_send.at[1], wo_recv.at[1], net.dev(SS))
    weight_sent = sends.settle()
    for h in range(heads):
        loads[h][4].wait()
    arrived(carry.at[c], state_recv.at[5])
    for h in range(heads):
        finished_head(h, 256, onward, rearward, inner, carry, og, head_gain, mixed)
        if h:
            sends.go(mixed.at[h - 1], mixed_x.at[h - 1], mix_send.at[h - 1], mix_recv.at[h - 1],
                     net.across())
    own_copies[0].wait()
    sends.go(mixed.at[heads - 1], mixed_x.at[heads - 1], mix_send.at[heads - 1],
             mix_recv.at[heads - 1], net.across())
    gate_a.far()
    gate_b.start()

    step = rows_in.shape[1]
    steps = rows // step

    def row_load(i, slot):
        return pltpu.make_async_copy(stream.at[pl.ds(pl.multiple_of(i * step, step), step)],
                                     rows_in.at[slot], row_sem.at[slot])

    def all_heads(ref, here):
        return jnp.concatenate([ref[h, here, :] for h in range(heads)], axis=1)

    def own_product(i, _):
        here = pl.ds(pl.multiple_of(i * step, step), step)
        normed[here, :] = product(all_heads(mixed, here),
                                  weight[pl.ds(mine_low, half), :]).astype(jnp.bfloat16)
        return 0

    row_load(0, 0).start()
    lax.fori_loop(0, steps, own_product, 0)
    up_a.near()
    cross_a.start()
    up_a.far()
    gate_a.hand_over()
    up_b.start()
    gate_b.near()
    cross_a.beside(0)
    up_a.hand_over()
    gate_b.far()
    cross_b.start()
    for h in range(heads):
        arrived(mixed_x.at[h], mix_recv.at[h])
    arrived(sib_part, wo_recv.at[1])

    def attend(i, _):
        slot = i % 2
        row_load(i, slot).wait()

        @pl.when(i + 1 < steps)
        def _():
            row_load(i + 1, 1 - slot).start()

        here = pl.ds(pl.multiple_of(i * step, step), step)
        away = product(all_heads(mixed_x, here),
                       weight[pl.ds(away_low, half), :]).astype(jnp.bfloat16)
        total = rows_in[slot].astype(jnp.float32) + (
            normed[here, :].astype(jnp.float32) + away.astype(jnp.float32))
        per = share // step

        @pl.when(i // per == t)
        def _():
            there = pl.ds(pl.multiple_of((i % per) * step, step), step)
            for n in range(resid.shape[0]):
                resid[n, there, :] = total[:, n * WIDE : (n + 1) * WIDE]

        factor = lax.rsqrt(jnp.mean(total * total, axis=-1, keepdims=True) + EPS)
        normed[here, :] = (total * factor * norm_gain[...]).astype(jnp.bfloat16)
        return 0

    lax.fori_loop(0, steps, attend, 0)
    cross_a.near()
    up_b.near()
    cross_b.beside(0)
    down_a.start()
    own_copies[1].wait()
    own_copies[2].wait()
    gate_a.siblings()
    up_a.siblings()

    columns = hidden.shape[1] // WIDE

    def wide_at(slot, n):
        return pl.ds(pl.multiple_of((slot * 2 + n) * WIDE, WIDE), WIDE)

    def wide_load(j, slot):
        there = pl.ds(pl.multiple_of(j * WIDE, WIDE), WIDE)
        return [pltpu.make_async_copy(full.at[:, there], weight.at[:, wide_at(slot, n)],
                                      wide_sem.at[slot, n])
                for n, full in enumerate((gate_full, up_full))]

    def hidden_block(end, j, _):
        slot = j % 2
        for copy in wide_load(j, slot):
            copy.wait()

        @pl.when(j + 1 < end)
        def _():
            for copy in wide_load(j + 1, 1 - slot):
                copy.start()

        there = pl.ds(pl.multiple_of(j * WIDE, WIDE), WIDE)

        def some(i, _):
            here = pl.ds(pl.multiple_of(i * share, share), share)
            g = product(normed[here, :], weight[:, wide_at(slot, 0)])
            u = product(normed[here, :], weight[:, wide_at(slot, 1)])
            hidden[here, there] = (g / (1.0 + jnp.exp(-g)) * u).astype(jnp.bfloat16)
            return 0

        lax.fori_loop(0, 2, some, 0)
        return 0

    def hidden_blocks(begin, end):
        for copy in wide_load(begin, begin % 2):
            copy.start()
        lax.fori_loop(begin, end, functools.partial(hidden_block, end), 0)

    weight_sent()
    cut = gate_a_columns // WIDE
    hidden_blocks(0, cut)
    up_b.far()
    cross_a.far()
    down_b.start()
    gate_b.hand_over()
    up_b.hand_over()
    cross_b.near()
    down_a.near()
    gate_b.siblings()
    up_b.siblings()
    hidden_blocks(cut, columns)
    down_b.near()
    cross_b.far()
    own_copies[3].wait()
    downs = (down_a, down_b, cross_a, cross_b)

    order = [(a, b) for a in range(planes) for b in range(2)]
    lanes = narrow.shape[2] // 2
    here = pl.ds(pl.multiple_of(t * share, share), share)
    there = pl.ds(pl.multiple_of((1 - t) * share, share), share)

    def narrow_load(n):
        pair = net.chip(order[n][0] * 4 + order[n][1] * 2) * 2
        return [pltpu.make_async_copy(down_full.at[pair + m],
                                      narrow.at[n % 2, :, m * lanes : (m + 1) * lanes],
                                      narrow_sem.at[n % 2, m]) for m in range(2)]

    for a in range(planes):
        if a == 3:
            down_a.far()
            down_b.far()
        down_a.beside(a)
        down_b.beside(a)
        for b in range(2):
            for p in downs:
                p.sibling(a, b)
            for copy in narrow_load(a * 2 + b):
                copy.start()
        for b in range(2):
            n = a * 2 + b
            for copy in narrow_load(n):
                copy.wait()
            part[n] = product(hidden[there, :], narrow[b]).astype(jnp.bfloat16)
            kept = product(hidden[here, :], narrow[b]).astype(jnp.bfloat16)
            sends.go(part.at[n], part_x.at[n], part_send.at[n], part_recv.at[n], net.across())
            block = net.chip(a * 4 + b * 2)
            resid[block] = resid[block] + kept.astype(jnp.float32)
    outs = []
    for n in range(len(order)):
        block = net.chip(order[n][0] * 4 + order[n][1] * 2)
        arrived(part_x.at[n], part_recv.at[n])
        part_x[n] = (resid[block] + part_x[n].astype(jnp.float32)).astype(jnp.bfloat16)
        out = pltpu.make_async_copy(
            part_x.at[n], result.at[:, pl.ds(pl.multiple_of(block * WIDE, WIDE), WIDE)], done_sem.at[n])
        out.start()
        outs.append(out)
    for out in outs:
        out.wait()
    sends.drain()


def pieces_of(units):
    half = (units // WIDE + 1) // 2 * WIDE
    pieces = [(w, a, b, False) for a, b in ((0, half), (half, units)) for w in "gu"]
    return pieces + [("d", units * i // 4, units * (i + 1) // 4, i >= 2) for i in range(4)]


def whole_layer(stream, queries, projected_keys, values, decay_gate_logits, decay_gate_bias,
                extra_log_decay, document_index, output_gate, head_norm_gain, output_weight,
                feedforward_norm_gain, gate_weight, up_weight, down_weight):
    heads = extra_log_decay.shape[1]
    rows, width = stream.shape
    dk = queries.shape[1] // heads
    dv = values.shape[1] // heads
    size = BLOCK_LENGTH
    blocks = rows // size
    devices = lax.axis_size("sp")
    planes = devices // 4
    share = rows // 2
    units = gate_weight.shape[1]
    chips = devices // 2
    decay = jax.nn.log_sigmoid(decay_gate_logits.astype(jnp.float32) + decay_gate_bias) / TAU
    decay = (decay.reshape(rows, heads, dk) + extra_log_decay[:, :, None]).reshape(rows, -1)
    doc = document_index.astype(jnp.float32)
    doc_wide = jnp.broadcast_to(doc[:, None], (rows, dk))
    doc_row = doc.reshape(blocks, size)
    pieces = pieces_of(units)
    any_, vm = pl.BlockSpec(memory_space=pl.ANY), pl.BlockSpec(memory_space=pltpu.VMEM)
    b16, f32 = jnp.bfloat16, jnp.float32
    dma = pltpu.SemaphoreType.DMA
    state = (heads, dk, dv)
    step = 256
    scratch = [
        pltpu.VMEM((heads, rows, dk), b16), pltpu.VMEM((heads, rows, dk), b16),
        pltpu.VMEM((heads, rows, dv), b16), pltpu.VMEM((heads, rows, dk), f32),
        pltpu.VMEM((rows, dk), f32), pltpu.VMEM((heads, rows, dv), b16),
        pltpu.VMEM((heads, rows, dk), b16), pltpu.VMEM((heads, rows, dk), b16),
        pltpu.VMEM((heads, rows, dv), f32), pltpu.VMEM((rows, dk), b16), pltpu.VMEM((rows, dk), b16),
        pltpu.VMEM((blocks, dk, dv), b16),
        pltpu.VMEM((2,) + state, b16), pltpu.VMEM((devices, 8, dk), f32),
        pltpu.VMEM(state, b16), pltpu.VMEM(state, b16), pltpu.VMEM(state, b16),
        pltpu.VMEM(state, b16), pltpu.VMEM(state, b16), pltpu.VMEM((planes - 1,) + state, b16),
        pltpu.VMEM((2,) + state, b16),
        pltpu.VMEM((heads, rows, dv), b16), pltpu.VMEM((heads, rows, dv), b16),
        pltpu.VMEM((2 * output_weight.shape[0], width), b16), pltpu.VMEM((rows, width), b16),
        pltpu.VMEM((chips, share, WIDE), f32), pltpu.VMEM((2, step, width), b16),
        pltpu.VMEM((rows, units), b16),
        pltpu.VMEM((2, units, WIDE), b16), pltpu.VMEM((chips, share, WIDE), b16),
        pltpu.VMEM((chips, share, WIDE), b16),
        dma((6, heads)), dma((4,)), dma((devices,)), dma((devices,)), dma((8,)), dma((8,)),
        dma((len(pieces), 24)), dma((len(pieces), devices)), dma((heads,)), dma((heads,)),
        dma((2,)), dma((2,)), dma((chips,)), dma((chips,)), dma((2,)), dma((2, 2)), dma((2, 2)),
        dma((chips,)),
    ]
    result = pl.pallas_call(
        functools.partial(layer_kernel, planes, size, pieces),
        out_shape=[
            jax.ShapeDtypeStruct(shape, b16)
            for shape in ((share, width), (devices * gate_weight.shape[0], units),
                          (devices * up_weight.shape[0], units), (devices,) + down_weight.shape)],
        in_specs=[any_] * 6 + [vm, any_, vm, any_, vm, any_, any_, any_],
        out_specs=[any_] * 4,
        scratch_shapes=scratch,
        compiler_params=pltpu.CompilerParams(collective_id=0, has_side_effects=True,
                                             vmem_limit_bytes=67043328),
        name="whole_layer",
    )(stream, queries, projected_keys, values, decay, doc_wide, doc_row, output_gate,
      head_norm_gain.astype(f32)[None], output_weight, feedforward_norm_gain.astype(f32)[None],
      gate_weight, up_weight, down_weight)
    return result[0]


def per_device(stream, queries, projected_keys, values, decay_gate_logits, decay_gate_bias,
               extra_log_decay, document_index, output_gate, head_norm_gain, output_weight,
               feedforward_norm_gain, gate_weight, up_weight, down_weight):
    tp = lax.axis_size("tp")
    if tp == 2 and lax.axis_size("sp") == 16:
        return whole_layer(
            stream, queries, projected_keys, values, decay_gate_logits, decay_gate_bias,
            extra_log_decay, document_index, output_gate, head_norm_gain, output_weight,
            feedforward_norm_gain, gate_weight, up_weight, down_weight)
    gather = lambda w, axis: lax.all_gather(w, "sp", axis=axis, tiled=True)
    gate_full = gather(gate_weight, 0)
    mixed, up_weight, gate_full = attention(
        queries, projected_keys, values, decay_gate_logits, decay_gate_bias, extra_log_decay,
        document_index, output_gate, head_norm_gain, up_weight, gate_full)
    up_full = gather(up_weight, 0)

    def hidden_of(normed):
        gate = product(normed, gate_full)
        up = product(normed, up_full)
        return (jax.nn.silu(gate) * up).astype(jnp.bfloat16)

    def down_of(hidden):
        return product(hidden, down_full).astype(jnp.bfloat16)

    share = stream.shape[0] // tp
    start = lax.axis_index("tp") * share
    own_stream = lax.dynamic_slice_in_dim(stream, start, share, 0).astype(jnp.float32)
    if tp == 2:
        swap = lambda x: lax.ppermute(x, "tp", [(0, 1), (1, 0)])
        chunks = 2
        step = share // chunks
        other = share - start
        rows_of = lambda x, base, c: lax.dynamic_slice_in_dim(x, base + c * step, step, 0)
        sent = [swap(product(rows_of(mixed, other, c), output_weight).astype(jnp.bfloat16))
                for c in range(chunks)]
        sent, up_full, down_weight = lax.optimization_barrier((sent, up_full, down_weight))
        down_full = gather(down_weight, 1)
        resid, normed = [], []
        for c in range(chunks):
            kept = product(rows_of(mixed, start, c), output_weight).astype(jnp.bfloat16)
            resid.append(own_stream[c * step : (c + 1) * step]
                         + (kept.astype(jnp.float32) + sent[c].astype(jnp.float32)))
            normed.append(row_norm(resid[c], feedforward_norm_gain))
        away = [swap(n) for n in normed]
        hidden_away = [hidden_of(n) for n in away]
        hidden_own = hidden_of(jnp.concatenate(normed))
        hidden_away, hidden_own, down_full = lax.optimization_barrier(
            (hidden_away, hidden_own, down_full))
        partial = [down_of(h) for h in hidden_away]
        partial, hidden_own = lax.optimization_barrier((partial, hidden_own))
        returned = [swap(p) for p in partial]
        kept = down_of(hidden_own)
        return jnp.concatenate([
            (resid[c] + (kept[c * step : (c + 1) * step].astype(jnp.float32)
                         + returned[c].astype(jnp.float32))).astype(jnp.bfloat16)
            for c in range(chunks)])
    down_full = gather(down_weight, 1)
    scatter = lambda x: lax.psum_scatter(x, "tp", scatter_dimension=0, tiled=True)
    attended = scatter(product(mixed, output_weight).astype(jnp.bfloat16)).astype(jnp.float32)
    resid = own_stream + attended
    normed = lax.all_gather(row_norm(resid, feedforward_norm_gain), "tp", axis=0, tiled=True)
    mlp_out = scatter(down_of(hidden_of(normed))).astype(jnp.float32)
    return (resid + mlp_out).astype(jnp.bfloat16)


def solution(mesh):
    placed = (
        P("sp", None),
        P("sp", "tp"),
        P("sp", "tp"),
        P("sp", "tp"),
        P("sp", "tp"),
        P("tp"),
        P("sp", "tp"),
        P("sp"),
        P("sp", "tp"),
        P(),
        P("tp", None),
        P(),
        P("sp", "tp"),
        P("sp", "tp"),
        P("tp", "sp"),
    )
    return jax.shard_map(
        per_device, mesh=mesh, in_specs=placed, out_specs=P(("sp", "tp"), None), check_vma=False
    )
```

```python
import functools

import jax
import jax.numpy as jnp
from jax import lax
from jax.experimental import pallas as pl
from jax.experimental.pallas import tpu as pltpu
from jax.sharding import PartitionSpec as P

BLOCK_LENGTH = 64
TAU = 16.0
EPS = 1e-06
HIGH = lax.Precision.HIGHEST
NT = (((1,), (1,)), ((), ()))
TN = (((0,), (0,)), ((), ()))


def shard_states(blocks, size, k_ref, v_ref, decay_ref, doc_ref, cum_ref, state_ref, log_ref,
                 tail_ref, lead_ref):
    rows = lax.broadcasted_iota(jnp.int32, (size, size), 0)
    cols = lax.broadcasted_iota(jnp.int32, (size, size), 1)
    lower = (cols <= rows).astype(jnp.float32)
    before = jnp.zeros((1, k_ref.shape[1]), jnp.float32)
    starts = []
    for b in range(blocks):
        here = pl.ds(b * size, size)
        cum = jnp.dot(lower, decay_ref[here, :], precision=HIGH,
                      preferred_element_type=jnp.float32)
        cum_ref[here, :] = cum
        starts.append(before)
        before = before + cum[size - 1 : size]
    total = before
    first = doc_ref[0:1, :]
    last = doc_ref[blocks * size - 1 : blocks * size, :]
    for b in range(blocks):
        here = pl.ds(b * size, size)
        cum = cum_ref[here, :] + starts[b]
        keys = k_ref[here, :].astype(jnp.float32)
        doc = doc_ref[here, :]
        tail_ref[here, :] = jnp.where(doc == last, keys * jnp.exp(total - cum), 0.0).astype(
            jnp.bfloat16)
        lead_ref[here, :] = jnp.where(doc == first, keys * jnp.exp(cum), 0.0).astype(
            jnp.bfloat16)
    values = v_ref[...]
    state_ref[0, 0] = lax.dot_general(
        tail_ref[...], values, TN, preferred_element_type=jnp.float32).astype(jnp.bfloat16)
    state_ref[1, 0] = lax.dot_general(
        lead_ref[...], values, TN, preferred_element_type=jnp.float32).astype(jnp.bfloat16)
    log_ref[0] = jnp.broadcast_to(total, log_ref.shape[1:])


def head_outputs(blocks, size, q_ref, k_ref, v_ref, cum_ref, doc_ref, same_ref, gate_ref,
                 gain_ref, carry_ref, out_ref, back_ref):
    scale = q_ref.shape[1] ** (-0.5)
    later = carry_ref[1, 0]
    for b in reversed(range(blocks)):
        here = pl.ds(b * size, size)
        back_ref[b] = later.astype(jnp.bfloat16)
        if b:
            cum = cum_ref[here, :]
            doc = doc_ref[here, :]
            first, last = doc[0:1], doc[size - 1 : size]
            previous = doc_ref[b * size - 1 : b * size, :]
            lead = jnp.where(doc == first, k_ref[here, :].astype(jnp.float32) * jnp.exp(cum), 0.0)
            added = lax.dot_general(lead.astype(jnp.bfloat16), v_ref[here, :], TN,
                                    preferred_element_type=jnp.float32)
            through = jnp.where(first == last, jnp.exp(cum[size - 1 : size]), 0.0)
            later = added + jnp.transpose(through) * later
            later = jnp.where(jnp.transpose(previous == first), later, 0.0)
    earlier = carry_ref[0, 0]
    rows = lax.broadcasted_iota(jnp.int32, (size, size), 0)
    cols = lax.broadcasted_iota(jnp.int32, (size, size), 1)
    for b in range(blocks):
        here = pl.ds(b * size, size)
        cum = cum_ref[here, :]
        doc = doc_ref[here, :]
        first, last = doc[0:1], doc[size - 1 : size]
        end = cum[size - 1 : size]
        query = q_ref[here, :].astype(jnp.float32) * scale
        keys = k_ref[here, :].astype(jnp.float32)
        values = v_ref[here, :]
        middle = cum[size // 2 - 1 : size // 2]
        rising = jnp.exp(cum - middle)
        falling = jnp.exp(middle - cum)
        forward = lax.dot_general((query * rising).astype(jnp.bfloat16),
                                  (keys * falling).astype(jnp.bfloat16), NT,
                                  preferred_element_type=jnp.float32)
        backward = lax.dot_general((query * falling).astype(jnp.bfloat16),
                                   (keys * rising).astype(jnp.bfloat16), NT,
                                   preferred_element_type=jnp.float32)
        same = same_ref[here, :] > 0.0
        scores = jnp.where(same & (cols <= rows), forward, 0.0) + jnp.where(
            same & (cols >= rows), backward, 0.0)
        total = jnp.dot(scores.astype(jnp.bfloat16), values, preferred_element_type=jnp.float32)
        shrink = jnp.exp(end - cum)
        onward = jnp.where(doc == first, query * jnp.exp(cum), 0.0).astype(jnp.bfloat16)
        rearward = jnp.where(doc == last, query * shrink, 0.0).astype(jnp.bfloat16)
        total = total + jnp.dot(onward, earlier.astype(jnp.bfloat16),
                                preferred_element_type=jnp.float32)
        total = total + jnp.dot(rearward, back_ref[b], preferred_element_type=jnp.float32)
        if b < blocks - 1:
            tail = jnp.where(doc == last, keys * shrink, 0.0)
            added = lax.dot_general(tail.astype(jnp.bfloat16), values, TN,
                                    preferred_element_type=jnp.float32)
            through = jnp.where(first == last, jnp.exp(end), 0.0)
            following = doc_ref[(b + 1) * size : (b + 1) * size + 1, :]
            earlier = added + jnp.transpose(through) * earlier
            earlier = jnp.where(jnp.transpose(last == following), earlier, 0.0)
        scaled = total * lax.rsqrt(jnp.mean(total * total, axis=-1, keepdims=True) + EPS)
        gate = gate_ref[here, :].astype(jnp.float32)
        scaled = scaled * gain_ref[...] * (gate / (1.0 + jnp.exp(-gate)))
        out_ref[here, :] = scaled.astype(jnp.bfloat16)


def row_norm(rows_f, gain):
    factor = lax.rsqrt(jnp.mean(rows_f * rows_f, axis=-1, keepdims=True) + EPS)
    return (rows_f * factor * gain.astype(jnp.float32)).astype(jnp.bfloat16)


def product(a, b):
    return jnp.dot(a, b, preferred_element_type=jnp.float32)


def carried_in(state, logs, leaves, enters, way):
    size = lax.axis_size("sp")
    me = lax.axis_index("sp")

    def from_away(distance, state, small):
        pairs = [(s, s + way * distance) for s in range(size) if 0 <= s + way * distance < size]
        return (lax.ppermute(state, "sp", pairs), lax.ppermute(small, "sp", pairs))

    def packed(logs, document):
        return jnp.concatenate([logs, jnp.full((1, logs.shape[1]), document)])

    state, small = from_away(1, state, packed(logs, leaves))
    place = me if way > 0 else size - 1 - me
    have = place >= 1
    state = jnp.where(have, state.astype(jnp.float32), 0.0)
    logs = jnp.where(have, small[:-1], 0.0)
    document = jnp.where(have, small[-1, 0], -1.0)
    distance = 1
    while distance < size - 1:
        far, small = from_away(distance, state.astype(jnp.bfloat16), packed(logs, document))
        reach = (place > distance) & (small[-1, 0] == document)
        weight = jnp.where(reach, jnp.exp(logs), 0.0)
        state = state + weight[..., None] * far.astype(jnp.float32)
        logs = logs + small[:-1]
        distance *= 2
    return jnp.where(document == enters, state, 0.0)


def attention(queries, projected_keys, values, decay_gate_logits, decay_gate_bias,
              extra_log_decay, document_index, output_gate, head_norm_gain, up_weight, gate_full):
    heads = extra_log_decay.shape[1]
    rows = queries.shape[0]
    dk = queries.shape[1] // heads
    dv = values.shape[1] // heads
    size = BLOCK_LENGTH
    blocks = rows // size
    decay = jax.nn.log_sigmoid(decay_gate_logits.astype(jnp.float32) + decay_gate_bias) / TAU
    decay = (decay.reshape(rows, heads, dk) + extra_log_decay[:, :, None]).reshape(rows, -1)
    doc = document_index.astype(jnp.float32)
    doc_wide = jnp.broadcast_to(doc[:, None], (rows, dk))
    by_block = doc.reshape(blocks, size)
    same = (by_block[:, :, None] == by_block[:, None, :]).astype(jnp.float32).reshape(rows, size)
    keyed = pl.BlockSpec((rows, dk), lambda h: (0, h))
    valued = pl.BlockSpec((rows, dv), lambda h: (0, h))
    fixed = pl.BlockSpec((rows, dk), lambda h: (0, 0))
    state_spec = pl.BlockSpec((2, 1, dk, dv), lambda h: (0, h, 0, 0))
    params = pltpu.CompilerParams(dimension_semantics=("arbitrary",),
                                  vmem_limit_bytes=40 * 1024 * 1024)
    cum, states, logs = pl.pallas_call(
        functools.partial(shard_states, blocks, size),
        grid=(heads,),
        out_shape=(
            jax.ShapeDtypeStruct((rows, heads * dk), jnp.float32),
            jax.ShapeDtypeStruct((2, heads, dk, dv), jnp.bfloat16),
            jax.ShapeDtypeStruct((heads, 8, dk), jnp.float32),
        ),
        in_specs=[keyed, valued, keyed, fixed],
        out_specs=(keyed, state_spec, pl.BlockSpec((1, 8, dk), lambda h: (h, 0, 0))),
        scratch_shapes=[pltpu.VMEM((rows, dk), jnp.bfloat16)] * 2,
        compiler_params=params,
        cost_estimate=pl.CostEstimate(flops=rows * heads * dk * dv * 4,
                                      bytes_accessed=rows * heads * dk * 20,
                                      transcendentals=rows * heads * dk * 2),
        name="shard_states",
    )(projected_keys, values, decay, doc_wide)
    first, last = doc[0], doc[rows - 1]
    logs = logs[:, 0]
    ahead = carried_in(states[0], logs, last, first, 1)
    ahead, up_weight, gate_full = lax.optimization_barrier((ahead, up_weight, gate_full))
    carry = jnp.stack([ahead, carried_in(states[1], logs, first, last, -1)])
    mixed = pl.pallas_call(
        functools.partial(head_outputs, blocks, size),
        grid=(heads,),
        out_shape=jax.ShapeDtypeStruct((rows, heads * dv), jnp.bfloat16),
        in_specs=[keyed, keyed, valued, keyed, fixed,
                  pl.BlockSpec((rows, size), lambda h: (0, 0)), valued,
                  pl.BlockSpec((1, dv), lambda h: (0, 0)), state_spec],
        out_specs=valued,
        scratch_shapes=[pltpu.VMEM((blocks, dk, dv), jnp.bfloat16)],
        compiler_params=params,
        cost_estimate=pl.CostEstimate(flops=rows * heads * dk * dv * 10,
                                      bytes_accessed=rows * heads * dk * 24,
                                      transcendentals=rows * heads * dk * 8),
        name="head_outputs",
    )(queries, projected_keys, values, cum, doc_wide, same, output_gate,
      head_norm_gain.astype(jnp.float32)[None], carry)
    return mixed, up_weight, gate_full


MESH = pl.DeviceIdType.MESH
Z1, Z2, Z3, YY, SS = 4, 8, 12, 2, 1
FIRST, LAST = 4, 5
WIDE = 256


class Net:
    def __init__(self, planes):
        place = lax.axis_index("sp")
        self.t = lax.axis_index("tp")
        self.c = place % 2
        self.y = (place // 2) % 2
        self.z = place // 4
        z = self.z
        self.zs = [z, z + 1 - 2 * (z % 2), (z + 2) % planes, planes - 1 - z]
        self.ys = [self.y, 1 - self.y]
        self.cs = [self.c, 1 - self.c]
        self.middle = (z == 1) | (z == 2)

    def chip(self, r):
        return self.zs[r // 4] * 2 + self.ys[(r // 2) % 2]

    def shard(self, r):
        return self.chip(r) * 2 + self.cs[r % 2]

    def dev(self, r):
        return (self.shard(r), self.t)

    def across(self):
        return (self.shard(0), 1 - self.t)


def maybe(cond, do):
    if cond is None:
        do()
    else:
        pl.when(cond)(do)


class Sends:
    def __init__(self):
        self.open = []

    def go(self, src, dst, send, recv, device, cond=None):
        copy = pltpu.make_async_remote_copy(src_ref=src, dst_ref=dst, send_sem=send, recv_sem=recv,
                                            device_id=device, device_id_type=MESH)
        maybe(cond, copy.start)
        self.open.append((copy, cond))

    def settle(self):
        copy, cond = self.open.pop()
        return functools.partial(maybe, cond, copy.wait_send)

    def drain(self):
        for copy, cond in self.open:
            maybe(cond, copy.wait_send)
        self.open = []


def arrived(ref, sem, cond=None):
    maybe(cond, pltpu.make_async_copy(ref, ref, sem).wait)


class Piece:
    def __init__(self, net, sends, own, full, recv, send, crossed):
        self.net, self.sends, self.own, self.full = net, sends, own, full
        self.recv, self.send, self.crossed, self.count = recv, send, crossed, 0

    def go(self, r, d, cond=None):
        dst = self.full(self.net.shard(r))
        self.sends.go(self.own if r == 0 else dst, dst, self.send.at[self.count],
                      self.recv.at[r ^ d], self.net.dev(d), cond)
        self.count += 1

    def wait(self, r):
        arrived(self.full(self.net.shard(r)), self.recv.at[r])

    def along(self, r):
        self.go(r, Z1)
        self.go(r, Z2)
        self.go(r, Z3, self.net.middle)

    def start_y(self):
        self.go(0, YY)
        self.go(0, SS)

    def start_z(self):
        self.along(0)

    def line(self, a):
        r = a * 4
        self.wait(r)
        if a == 2:
            self.go(r, Z1, self.net.middle)
        if not self.crossed:
            self.go(r, YY)
        self.go(r, SS)

    def beside(self, a):
        r = a * 4 + YY
        self.wait(r)
        if self.crossed:
            if a == 0:
                self.along(r)
            if a == 2:
                self.go(r, Z1, self.net.middle)
        self.go(r, SS)

    def siblings(self):
        for a in range(4):
            for b in range(2):
                self.sibling(a, b)

    def sibling(self, a, b):
        self.wait(a * 4 + b * 2 + 1)


def column(rows, h):
    return jnp.transpose(rows)[:, h : h + 1]


def document_columns(blocks, size, doc_line, doc, doc_row):
    rows = lax.broadcasted_iota(jnp.int32, (size, size), 0)
    cols = lax.broadcasted_iota(jnp.int32, (size, size), 1)
    for b in range(blocks):
        line = doc_line[0:1, b * size : (b + 1) * size].astype(jnp.float32)
        doc_row[b : b + 1, :] = line
        column = jnp.sum(jnp.where(rows == cols, line, 0.0), axis=1, keepdims=True)
        doc[pl.ds(b * size, size), :] = jnp.broadcast_to(column, (size, doc.shape[1]))


def prefix_sums(blocks, size, h, logits, bias, extra, cums, table):
    rows = lax.broadcasted_iota(jnp.int32, (size, size), 0)
    cols = lax.broadcasted_iota(jnp.int32, (size, size), 1)
    lower = (cols <= rows).astype(jnp.float32)
    total = jnp.zeros((1, cums.shape[2]), jnp.float32)
    shift = bias[pl.ds(h, 1), :]
    line = extra[pl.ds(h, 1), :]
    for b in range(blocks):
        here = pl.ds(b * size, size)
        x = logits[h, here, :].astype(jnp.float32) + shift
        decay = (jnp.minimum(x, 0.0) - jnp.log1p(jnp.exp(-jnp.abs(x)))) / TAU
        added = line[:, b * size : (b + 1) * size]
        cum = jnp.dot(lower, decay, precision=HIGH, preferred_element_type=jnp.float32)
        cum = cum + jnp.sum(lower * added, axis=1, keepdims=True)
        cums[h, here, :] = cum
        total = total + cum[size - 1 : size]
    table[0, pl.ds(h, 1), :] = total


def own_states(blocks, size, h, q, k, v, cums, doc, table, onward, rearward, tail, lead, states):
    scale = q.shape[2] ** (-0.5)
    total = table[0, pl.ds(h, 1), :]
    first = doc[0:1, :]
    last = doc[blocks * size - 1 : blocks * size, :]
    before = jnp.zeros_like(total)
    for b in range(blocks):
        here = pl.ds(b * size, size)
        inner = cums[h, here, :]
        cum = inner + before
        before = before + inner[size - 1 : size]
        keys = k[h, here, :].astype(jnp.float32)
        query = q[h, here, :].astype(jnp.float32) * scale
        docs = doc[here, :]
        grown = jnp.where(docs == first, jnp.exp(cum), 0.0)
        shrunk = jnp.where(docs == last, jnp.exp(total - cum), 0.0)
        tail[here, :] = (keys * shrunk).astype(jnp.bfloat16)
        lead[here, :] = (keys * grown).astype(jnp.bfloat16)
        onward[h, here, :] = (query * grown).astype(jnp.bfloat16)
        rearward[h, here, :] = (query * shrunk).astype(jnp.bfloat16)
    values = v[h]
    states[0, h] = lax.dot_general(tail[...], values, TN,
                                   preferred_element_type=jnp.float32).astype(jnp.bfloat16)
    states[1, h] = lax.dot_general(lead[...], values, TN,
                                   preferred_element_type=jnp.float32).astype(jnp.bfloat16)


def inner_outputs(blocks, size, h, q, k, v, cums, doc, doc_row, back, out):
    scale = q.shape[2] ** (-0.5)
    rows = lax.broadcasted_iota(jnp.int32, (size, size), 0)
    cols = lax.broadcasted_iota(jnp.int32, (size, size), 1)
    later = jnp.zeros((k.shape[2], v.shape[2]), jnp.float32)
    for b in reversed(range(blocks)):
        here = pl.ds(b * size, size)
        back[b] = later.astype(jnp.bfloat16)
        if b:
            cum = cums[h, here, :]
            docs = doc[here, :]
            first, last = docs[0:1], docs[size - 1 : size]
            previous = doc[b * size - 1 : b * size, :]
            grown = jnp.where(docs == first, k[h, here, :].astype(jnp.float32) * jnp.exp(cum), 0.0)
            added = lax.dot_general(grown.astype(jnp.bfloat16), v[h, here, :], TN,
                                    preferred_element_type=jnp.float32)
            through = jnp.where(first == last, jnp.exp(cum[size - 1 : size]), 0.0)
            later = added + jnp.transpose(through) * later
            later = jnp.where(jnp.transpose(previous == first), later, 0.0)
    earlier = jnp.zeros((k.shape[2], v.shape[2]), jnp.float32)
    for b in range(blocks):
        here = pl.ds(b * size, size)
        cum = cums[h, here, :]
        docs = doc[here, :]
        first, last = docs[0:1], docs[size - 1 : size]
        end = cum[size - 1 : size]
        query = q[h, here, :].astype(jnp.float32) * scale
        keys = k[h, here, :].astype(jnp.float32)
        values = v[h, here, :]
        middle = cum[size // 2 - 1 : size // 2]
        rising = jnp.exp(cum - middle)
        falling = jnp.exp(middle - cum)
        forward = lax.dot_general((query * rising).astype(jnp.bfloat16),
                                  (keys * falling).astype(jnp.bfloat16), NT,
                                  preferred_element_type=jnp.float32)
        backward = lax.dot_general((query * falling).astype(jnp.bfloat16),
                                   (keys * rising).astype(jnp.bfloat16), NT,
                                   preferred_element_type=jnp.float32)
        same = docs[:, :size] == doc_row[b : b + 1, :]
        scores = jnp.where(same & (cols <= rows), forward, 0.0) + jnp.where(
            same & (cols >= rows), backward, 0.0)
        total = jnp.dot(scores.astype(jnp.bfloat16), values, preferred_element_type=jnp.float32)
        shrink = jnp.exp(end - cum)
        if b:
            onward = jnp.where(docs == first, query * jnp.exp(cum), 0.0).astype(jnp.bfloat16)
            total = total + jnp.dot(onward, earlier.astype(jnp.bfloat16),
                                    preferred_element_type=jnp.float32)
        if b < blocks - 1:
            rearward = jnp.where(docs == last, query * shrink, 0.0).astype(jnp.bfloat16)
            total = total + jnp.dot(rearward, back[b], preferred_element_type=jnp.float32)
            tail = jnp.where(docs == last, keys * shrink, 0.0)
            added = lax.dot_general(tail.astype(jnp.bfloat16), values, TN,
                                    preferred_element_type=jnp.float32)
            through = jnp.where(first == last, jnp.exp(end), 0.0)
            following = doc[(b + 1) * size : (b + 1) * size + 1, :]
            earlier = added + jnp.transpose(through) * earlier
            earlier = jnp.where(jnp.transpose(last == following), earlier, 0.0)
        out[h, here, :] = total


def finished_head(h, step, onward, rearward, inner, carry, gate, gain, mixed):
    def some(i, _):
        here = pl.ds(pl.multiple_of(i * step, step), step)
        total = inner[h, here, :]
        total = total + jnp.dot(onward[h, here, :], carry[0, h], preferred_element_type=jnp.float32)
        total = total + jnp.dot(rearward[h, here, :], carry[1, h],
                                preferred_element_type=jnp.float32)
        scaled = total * lax.rsqrt(jnp.mean(total * total, axis=-1, keepdims=True) + EPS)
        g = gate[h, here, :].astype(jnp.float32)
        mixed[h, here, :] = (scaled * gain[...] * (g / (1.0 + jnp.exp(-g)))).astype(jnp.bfloat16)
        return 0

    lax.fori_loop(0, inner.shape[1] // step, some, 0)


def layer_kernel(planes, size, pieces, plan, groups,
                 stream, queries, keys, values, logits_w, bias, extra, doc_line, out_gate, head_gain,
                 out_weight, norm_gain, gate_w, up_w, down_w,
                 result, gate_full, up_full, down_full,
                 q, k, v, logits, cums, doc, doc_row, og, onward, rearward, inner, tail, lead, back,
                 states, table, chip_state, plane_state, chip_carry, from_sib, from_y, from_z, carry,
                 mixed, mixed_x, weight, normed, resid, rows_in, hidden, narrow, part, part_x, kept,
                 load_sem, own_sem, table_send, table_recv, state_send, state_recv,
                 piece_send, piece_recv, mix_send, mix_recv, wo_send, wo_recv, part_send, part_recv,
                 row_sem, wide_sem, narrow_sem, done_sem):
    net = Net(planes)
    sends = Sends()
    heads, rows, dk = q.shape
    dv = v.shape[2]
    blocks = rows // size
    c, y, z, t = net.c, net.y, net.z, net.t
    half = out_weight.shape[0]
    quarter = half // 2
    share = rows // 2

    loads = []
    for h in range(heads):
        group = []
        for n, (src, dst, width) in enumerate(((logits_w, logits, dk), (keys, k, dk), (queries, q, dk),
                                               (values, v, dv), (out_gate, og, dv))):
            group.append(pltpu.make_async_copy(src.at[:, h * width : (h + 1) * width], dst.at[h],
                                               load_sem.at[n, h]))
        loads.append(group)
    for n in range(4):
        for h in range(heads):
            loads[h][n].start()
    for h in range(heads):
        loads[h][4].start()

    barrier = pltpu.get_barrier_semaphore()
    for r in range(1, 4 * planes):
        pl.semaphore_signal(barrier, inc=1, device_id=net.dev(r), device_id_type=MESH)
    pl.semaphore_signal(barrier, inc=1, device_id=net.across(), device_id_type=MESH)
    pl.semaphore_wait(barrier, 4 * planes)

    shards = {"g": (gate_w, gate_full), "u": (up_w, up_full), "d": (down_w, down_full)}

    def place(full, low, high, shard):
        if len(full.shape) == 3:
            return full.at[shard, low:high]
        own = full.shape[0] // (4 * planes)
        return full.at[pl.ds(pl.multiple_of(shard * own, own), own), low:high]

    ps = []
    for i, (name, low, high, crossed) in enumerate(pieces):
        own, full = shards[name]
        mine = own.at[low:high] if len(full.shape) == 3 else own.at[:, low:high]
        ps.append(Piece(net, sends, mine, functools.partial(place, full, low, high),
                        piece_recv.at[i], piece_send.at[i], crossed))
    downs = [p for p, (name, _, _, _) in zip(ps, pieces) if name == "d"]
    gaps = iter(plan)

    def tasks():
        for kind, i, a in next(gaps):
            if kind == 0:
                ps[i].start_y()
            elif kind == 1:
                ps[i].start_z()
            elif kind == 2:
                ps[i].line(a)
            else:
                ps[i].beside(a)

    tasks()
    mine_low = pl.multiple_of(t * half, half)
    away_low = pl.multiple_of((1 - t) * half, half)
    sends.go(out_weight.at[pl.ds(pl.multiple_of(c * quarter, quarter), quarter)],
             weight.at[pl.ds(pl.multiple_of(t * half + c * quarter, quarter), quarter)],
             wo_send.at[0], wo_recv.at[0], net.across())
    own_copies = [pltpu.make_async_copy(out_weight, weight.at[pl.ds(mine_low, half)], own_sem.at[0])]
    me = net.shard(0)
    for i, (own, full) in enumerate(shards.values()):
        own_copies.append(pltpu.make_async_copy(
            own, place(full, 0, own.shape[len(full.shape) == 2], me), own_sem.at[i + 1]))

    document_columns(blocks, size, doc_line, doc, doc_row)
    for h in range(heads):
        loads[h][0].wait()
    table[0] = jnp.where(
        lax.broadcasted_iota(jnp.int32, table.shape[1:], 0) == FIRST,
        jnp.broadcast_to(doc[0:1, :], table.shape[1:]),
        jnp.broadcast_to(doc[rows - 1 : rows, :], table.shape[1:]))

    def sums(h, _):
        prefix_sums(blocks, size, h, logits, bias, extra, cums, table)
        return 0

    lax.fori_loop(0, heads, sums, 0)
    for h in range(heads):
        for n in (1, 2, 3):
            loads[h][n].wait()

    def state_of(h, _):
        own_states(blocks, size, h, q, k, v, cums, doc, table, onward, rearward, tail, lead, states)
        return 0

    lax.fori_loop(0, heads, state_of, 0)
    sends.go(table.at[0], table.at[1], table_send.at[0], table_recv.at[0], net.dev(SS))
    sends.go(states.at[c], from_sib, state_send.at[0], state_recv.at[0], net.dev(SS))
    for copy in own_copies:
        copy.start()

    def state(r):
        return table[r]

    rising = c == 1

    def leaves(r):
        return jnp.where(rising, state(r)[LAST : LAST + 1], state(r)[FIRST : FIRST + 1])

    def enters(r):
        return jnp.where(rising, state(r)[FIRST : FIRST + 1], state(r)[LAST : LAST + 1])

    def chip_log(r):
        return state(r) + state(r ^ 1)

    def plane_log(a):
        return chip_log(a * 4) + chip_log(a * 4 + 2)

    arrived(table.at[1], table_recv.at[0])
    sends.go(table.at[0:2], table.at[2:4], table_send.at[1], table_recv.at[1], net.dev(YY))
    arrived(from_sib, state_recv.at[0])
    fade = jnp.where(leaves(1) == leaves(0), jnp.exp(state(0)), 0.0)
    way = 1 - c
    for h in range(heads):
        chip_state[h] = (states[way, h].astype(jnp.float32)
                         + column(fade, h) * from_sib[h].astype(jnp.float32)).astype(jnp.bfloat16)
    tasks()
    sends.go(chip_state, from_y, state_send.at[1], state_recv.at[1], net.dev(YY))

    def inner_of(h, _):
        inner_outputs(blocks, size, h, q, k, v, cums, doc, doc_row, back, inner)
        return 0

    tasks()
    lax.fori_loop(0, 2, inner_of, 0)
    tasks()
    arrived(table.at[2:4], table_recv.at[1])
    arrived(from_y, state_recv.at[1])
    tasks()
    upper = y == c
    fade = jnp.where(leaves(2) == leaves(0),
                     jnp.exp(jnp.where(upper, chip_log(0), chip_log(2))), 0.0)
    for h in range(heads):
        mine = chip_state[h].astype(jnp.float32)
        other = from_y[h].astype(jnp.float32)
        high = jnp.where(upper, mine, other)
        low = jnp.where(upper, other, mine)
        plane_state[h] = (high + column(fade, h) * low).astype(jnp.bfloat16)
    tasks()
    early, late = [None], [None]
    for a in range(1, planes):
        below = net.zs[a] < z
        early.append((rising & below) | ((c == 0) & (net.zs[a] > z)))
        late.append((rising & (net.zs[a] > z)) | ((c == 0) & below))
    for a in range(1, planes):
        sends.go(table.at[0:4], table.at[a * 4 : a * 4 + 4], table_send.at[1 + a],
                 table_recv.at[1 + a], net.dev(a * 4), late[a])
        sends.go(plane_state, from_z.at[a - 1], state_send.at[1 + a], state_recv.at[1 + a],
                 net.dev(a * 4), late[a])
    tasks()
    lax.fori_loop(2, heads, inner_of, 0)
    tasks()
    for a in range(1, planes):
        arrived(table.at[a * 4 : a * 4 + 4], table_recv.at[1 + a], early[a])
        arrived(from_z.at[a - 1], state_recv.at[1 + a], early[a])
    entry = enters(1)
    fades = []
    for a in range(1, planes):
        log = jnp.where(upper, chip_log(2), 0.0)
        for b in range(1, planes):
            if b != a:
                between = (net.zs[b] - net.zs[a]) * (z - net.zs[b]) > 0
                log = log + jnp.where(between, plane_log(b), 0.0)
        out_doc = jnp.where(upper, leaves(a * 4), leaves(a * 4 + 2))
        fades.append(jnp.where((out_doc == entry) & early[a], jnp.exp(log), 0.0))
    joins = jnp.where((leaves(2) == entry) & upper, jnp.ones_like(entry), 0.0)
    joins = jnp.broadcast_to(joins, (8, dk))
    through = jnp.where(enters(1) == leaves(1), jnp.exp(state(1)), 0.0)
    joined = jnp.broadcast_to(jnp.where(leaves(1) == enters(0), jnp.ones_like(entry), 0.0), (8, dk))
    for h in range(heads):
        into = column(joins, h) * from_y[h].astype(jnp.float32)
        for a in range(1, planes):
            into = into + column(fades[a - 1], h) * jnp.where(
                early[a], from_z[a - 1, h].astype(jnp.float32), 0.0)
        chip_carry[h] = into.astype(jnp.bfloat16)
        carry[way, h] = (column(joined, h) * (from_sib[h].astype(jnp.float32)
                                              + column(through, h) * into)).astype(jnp.bfloat16)
    sends.go(chip_carry, carry.at[way], state_send.at[5], state_recv.at[5], net.dev(SS))
    own_part = weight.at[pl.ds(pl.multiple_of((1 - t) * half + c * quarter, quarter), quarter)]
    sib_part = weight.at[pl.ds(pl.multiple_of((1 - t) * half + (1 - c) * quarter, quarter), quarter)]
    for h in range(heads):
        loads[h][4].wait()
    arrived(carry.at[c], state_recv.at[5])
    tasks()

    def mix_send_of(h):
        sends.go(mixed.at[h], mixed_x.at[h], mix_send.at[h], mix_recv.at[h], net.across())

    for h in range(heads):
        finished_head(h, 256, onward, rearward, inner, carry, og, head_gain, mixed)
        tasks()
        if h:
            mix_send_of(h - 1)
        tasks()
    own_copies[0].wait()
    mix_send_of(heads - 1)

    step = rows_in.shape[1]
    steps = rows // step

    def row_load(i, slot):
        return pltpu.make_async_copy(stream.at[pl.ds(pl.multiple_of(i * step, step), step)],
                                     rows_in.at[slot], row_sem.at[slot])

    def all_heads(ref, here):
        return jnp.concatenate([ref[h, here, :] for h in range(heads)], axis=1)

    def own_product(i, _):
        here = pl.ds(pl.multiple_of(i * step, step), step)
        normed[here, :] = product(all_heads(mixed, here),
                                  weight[pl.ds(mine_low, half), :]).astype(jnp.bfloat16)
        return 0

    row_load(0, 0).start()
    lax.fori_loop(0, steps, own_product, 0)
    tasks()
    arrived(own_part, wo_recv.at[0])
    sends.go(own_part, own_part, wo_send.at[1], wo_recv.at[1], net.dev(SS))
    weight_sent = sends.settle()
    for h in range(heads):
        arrived(mixed_x.at[h], mix_recv.at[h])
    arrived(sib_part, wo_recv.at[1])
    tasks()

    def attend(i, _):
        slot = i % 2
        row_load(i, slot).wait()

        @pl.when(i + 1 < steps)
        def _():
            row_load(i + 1, 1 - slot).start()

        here = pl.ds(pl.multiple_of(i * step, step), step)
        away = product(all_heads(mixed_x, here),
                       weight[pl.ds(away_low, half), :]).astype(jnp.bfloat16)
        total = rows_in[slot].astype(jnp.float32) + (
            normed[here, :].astype(jnp.float32) + away.astype(jnp.float32))
        per = share // step

        @pl.when(i // per == t)
        def _():
            there = pl.ds(pl.multiple_of((i % per) * step, step), step)
            for n in range(resid.shape[0]):
                resid[n, there, :] = total[:, n * WIDE : (n + 1) * WIDE]

        factor = lax.rsqrt(jnp.mean(total * total, axis=-1, keepdims=True) + EPS)
        normed[here, :] = (total * factor * norm_gain[...]).astype(jnp.bfloat16)
        return 0

    lax.fori_loop(0, steps, attend, 0)
    tasks()
    own_copies[1].wait()
    own_copies[2].wait()
    weight_sent()


    def wide_at(slot, n):
        return pl.ds(pl.multiple_of((slot * 2 + n) * WIDE, WIDE), WIDE)

    def wide_load(j, slot):
        there = pl.ds(pl.multiple_of(j * WIDE, WIDE), WIDE)
        return [pltpu.make_async_copy(full.at[:, there], weight.at[:, wide_at(slot, n)],
                                      wide_sem.at[slot, n])
                for n, full in enumerate((gate_full, up_full))]

    def hidden_block(end, j, _):
        slot = j % 2
        for copy in wide_load(j, slot):
            copy.wait()

        @pl.when(j + 1 < end)
        def _():
            for copy in wide_load(j + 1, 1 - slot):
                copy.start()

        there = pl.ds(pl.multiple_of(j * WIDE, WIDE), WIDE)

        def some(i, _):
            here = pl.ds(pl.multiple_of(i * share, share), share)
            g = product(normed[here, :], weight[:, wide_at(slot, 0)])
            u = product(normed[here, :], weight[:, wide_at(slot, 1)])
            hidden[here, there] = (g / (1.0 + jnp.exp(-g)) * u).astype(jnp.bfloat16)
            return 0

        lax.fori_loop(0, 2, some, 0)
        return 0

    def hidden_blocks(begin, end):
        for copy in wide_load(begin, begin % 2):
            copy.start()
        lax.fori_loop(begin, end, functools.partial(hidden_block, end), 0)

    for needs, begin, end in groups:
        for i in needs:
            ps[i].siblings()
        hidden_blocks(begin, end)
        tasks()
    own_copies[3].wait()

    order = [(a, b) for a in range(planes) for b in range(2)]
    lanes = narrow.shape[2] // 2
    here = pl.ds(pl.multiple_of(t * share, share), share)
    there = pl.ds(pl.multiple_of((1 - t) * share, share), share)
    for n, (a, b) in enumerate(order):
        for p in downs:
            p.sibling(a, b)
        block = net.chip(a * 4 + b * 2)
        last_block = net.chip(order[n - 1][0] * 4 + order[n - 1][1] * 2)
        copies = [pltpu.make_async_copy(down_full.at[block * 2 + m],
                                        narrow.at[b, :, m * lanes : (m + 1) * lanes],
                                        narrow_sem.at[b, m]) for m in range(2)]
        for copy in copies:
            copy.start()
        if n:
            kept[...] = product(hidden[here, :], narrow[1 - b]).astype(jnp.bfloat16)
        for copy in copies:
            copy.wait()
        part[n] = product(hidden[there, :], narrow[b]).astype(jnp.bfloat16)
        if n:
            resid[last_block] = resid[last_block] + kept[...].astype(jnp.float32)
        sends.go(part.at[n], part_x.at[n], part_send.at[n], part_recv.at[n], net.across())
        tasks()
    block = net.chip(order[-1][0] * 4 + order[-1][1] * 2)
    away = product(hidden[here, :], narrow[order[-1][1]]).astype(jnp.bfloat16)
    resid[block] = resid[block] + away.astype(jnp.float32)
    outs = []
    for n in range(len(order)):
        block = net.chip(order[n][0] * 4 + order[n][1] * 2)
        arrived(part_x.at[n], part_recv.at[n])
        part_x[n] = (resid[block] + part_x[n].astype(jnp.float32)).astype(jnp.bfloat16)
        out = pltpu.make_async_copy(
            part_x.at[n], result.at[:, pl.ds(pl.multiple_of(block * WIDE, WIDE), WIDE)], done_sem.at[n])
        out.start()
        outs.append(out)
    for out in outs:
        out.wait()
    sends.drain()


PLAN = (
    ((1, 0, 0), (0, 0, 0),),
    (),
    (),
    (),
    ((0, 1, 0),),
    (),
    ((2, 0, 1), (1, 1, 0), (2, 0, 2),),
    ((0, 5, 0), (0, 6, 0), (2, 0, 3),),
    (),
    ((3, 1, 0), (0, 3, 0),),
    ((1, 2, 0),),
    (),
    ((0, 2, 0),),
    (),
    ((1, 3, 0),),
    (),
    ((2, 1, 1),),
    ((1, 5, 0), (3, 0, 1), (3, 0, 3), (3, 0, 2), (3, 0, 0), (2, 1, 2), (2, 2, 1), (3, 3, 0), (2, 1, 3), (3, 1, 1), (2, 2, 2),),
    ((2, 2, 3),),
    ((3, 1, 2), (2, 3, 1), (3, 1, 3), (2, 3, 2), (1, 4, 0),),
    (),
    ((3, 5, 0), (3, 2, 0), (2, 3, 3), (2, 5, 1),),
    ((3, 3, 3), (0, 4, 0), (1, 6, 0), (3, 6, 0), (3, 2, 1), (3, 2, 3), (3, 3, 1), (3, 3, 2), (2, 5, 2), (3, 2, 2),),
    ((3, 5, 1),),
    (),
    ((3, 4, 0),),
    ((2, 4, 1),),
    ((2, 4, 2), (2, 5, 3), (2, 6, 1),),
    ((3, 4, 1), (2, 6, 2), (3, 5, 2), (3, 4, 2), (3, 6, 1),),
    (),
    ((2, 4, 3), (3, 6, 2), (2, 6, 3), (3, 4, 3),),
    (),
    ((3, 6, 3), (3, 5, 3),),
    (),
)


def pieces_of(units):
    block = units // 11
    pieces = [
        ("g", block * 0, block * 6, False),
        ("u", block * 0, block * 6, False),
        ("g", block * 6, block * 11, False),
        ("u", block * 6, block * 11, False),
        ("d", units * 0 // 176, units * 66 // 176, False),
        ("d", units * 66 // 176, units * 132 // 176, False),
        ("d", units * 132 // 176, units * 176 // 176, True),
    ]
    groups = (
        ((0, 1), 0, 2),
        ((), 2, 4),
        ((), 4, 6),
        ((2, 3), 6, 8),
        ((), 8, 10),
        ((), 10, 11),
    )
    return pieces, groups

def whole_layer(stream, queries, projected_keys, values, decay_gate_logits, decay_gate_bias,
                extra_log_decay, document_index, output_gate, head_norm_gain, output_weight,
                feedforward_norm_gain, gate_weight, up_weight, down_weight):
    heads = extra_log_decay.shape[1]
    rows, width = stream.shape
    dk = queries.shape[1] // heads
    dv = values.shape[1] // heads
    size = BLOCK_LENGTH
    blocks = rows // size
    devices = lax.axis_size("sp")
    planes = devices // 4
    share = rows // 2
    units = gate_weight.shape[1]
    chips = devices // 2
    pieces, groups = pieces_of(units)
    any_, vm = pl.BlockSpec(memory_space=pl.ANY), pl.BlockSpec(memory_space=pltpu.VMEM)
    b16, f32 = jnp.bfloat16, jnp.float32
    dma = pltpu.SemaphoreType.DMA
    state = (heads, dk, dv)
    step = 256
    scratch = [
        pltpu.VMEM((heads, rows, dk), b16), pltpu.VMEM((heads, rows, dk), b16),
        pltpu.VMEM((heads, rows, dv), b16), pltpu.VMEM((heads, rows, dk), b16),
        pltpu.VMEM((heads, rows, dk), f32), pltpu.VMEM((rows, dk), f32),
        pltpu.VMEM((blocks, size), f32), pltpu.VMEM((heads, rows, dv), b16),
        pltpu.VMEM((heads, rows, dk), b16), pltpu.VMEM((heads, rows, dk), b16),
        pltpu.VMEM((heads, rows, dv), f32), pltpu.VMEM((rows, dk), b16), pltpu.VMEM((rows, dk), b16),
        pltpu.VMEM((blocks, dk, dv), b16),
        pltpu.VMEM((2,) + state, b16), pltpu.VMEM((devices, 8, dk), f32),
        pltpu.VMEM(state, b16), pltpu.VMEM(state, b16), pltpu.VMEM(state, b16),
        pltpu.VMEM(state, b16), pltpu.VMEM(state, b16), pltpu.VMEM((planes - 1,) + state, b16),
        pltpu.VMEM((2,) + state, b16),
        pltpu.VMEM((heads, rows, dv), b16), pltpu.VMEM((heads, rows, dv), b16),
        pltpu.VMEM((2 * output_weight.shape[0], width), b16), pltpu.VMEM((rows, width), b16),
        pltpu.VMEM((chips, share, WIDE), f32), pltpu.VMEM((2, step, width), b16),
        pltpu.VMEM((rows, units), b16),
        pltpu.VMEM((2, units, WIDE), b16), pltpu.VMEM((chips, share, WIDE), b16),
        pltpu.VMEM((chips, share, WIDE), b16), pltpu.VMEM((share, WIDE), b16),
        dma((6, heads)), dma((4,)), dma((8,)), dma((8,)), dma((8,)), dma((8,)),
        dma((len(pieces), 24)), dma((len(pieces), devices)), dma((heads,)), dma((heads,)),
        dma((2,)), dma((2,)), dma((chips,)), dma((chips,)), dma((2,)), dma((2, 2)), dma((2, 2)),
        dma((chips,)),
    ]
    result = pl.pallas_call(
        functools.partial(layer_kernel, planes, size, pieces, PLAN, groups),
        out_shape=[
            jax.ShapeDtypeStruct(shape, b16)
            for shape in ((share, width), (devices * gate_weight.shape[0], units),
                          (devices * up_weight.shape[0], units), (devices,) + down_weight.shape)],
        in_specs=[any_] * 5 + [vm, vm, vm, any_, vm, any_, vm, any_, any_, any_],
        out_specs=[any_] * 4,
        scratch_shapes=scratch,
        compiler_params=pltpu.CompilerParams(collective_id=0, has_side_effects=True,
                                             vmem_limit_bytes=67043328),
        name="whole_layer",
    )(stream, queries, projected_keys, values, decay_gate_logits,
      decay_gate_bias.reshape(heads, dk), extra_log_decay.T, document_index[None], output_gate,
      head_norm_gain.astype(f32)[None], output_weight, feedforward_norm_gain.astype(f32)[None],
      gate_weight, up_weight, down_weight)
    return result[0]


def per_device(stream, queries, projected_keys, values, decay_gate_logits, decay_gate_bias,
               extra_log_decay, document_index, output_gate, head_norm_gain, output_weight,
               feedforward_norm_gain, gate_weight, up_weight, down_weight):
    tp = lax.axis_size("tp")
    if tp == 2 and lax.axis_size("sp") == 16:
        return whole_layer(
            stream, queries, projected_keys, values, decay_gate_logits, decay_gate_bias,
            extra_log_decay, document_index, output_gate, head_norm_gain, output_weight,
            feedforward_norm_gain, gate_weight, up_weight, down_weight)
    gather = lambda w, axis: lax.all_gather(w, "sp", axis=axis, tiled=True)
    gate_full = gather(gate_weight, 0)
    mixed, up_weight, gate_full = attention(
        queries, projected_keys, values, decay_gate_logits, decay_gate_bias, extra_log_decay,
        document_index, output_gate, head_norm_gain, up_weight, gate_full)
    up_full = gather(up_weight, 0)

    def hidden_of(normed):
        gate = product(normed, gate_full)
        up = product(normed, up_full)
        return (jax.nn.silu(gate) * up).astype(jnp.bfloat16)

    def down_of(hidden):
        return product(hidden, down_full).astype(jnp.bfloat16)

    share = stream.shape[0] // tp
    start = lax.axis_index("tp") * share
    own_stream = lax.dynamic_slice_in_dim(stream, start, share, 0).astype(jnp.float32)
    if tp == 2:
        swap = lambda x: lax.ppermute(x, "tp", [(0, 1), (1, 0)])
        chunks = 2
        step = share // chunks
        other = share - start
        rows_of = lambda x, base, c: lax.dynamic_slice_in_dim(x, base + c * step, step, 0)
        sent = [swap(product(rows_of(mixed, other, c), output_weight).astype(jnp.bfloat16))
                for c in range(chunks)]
        sent, up_full, down_weight = lax.optimization_barrier((sent, up_full, down_weight))
        down_full = gather(down_weight, 1)
        resid, normed = [], []
        for c in range(chunks):
            kept = product(rows_of(mixed, start, c), output_weight).astype(jnp.bfloat16)
            resid.append(own_stream[c * step : (c + 1) * step]
                         + (kept.astype(jnp.float32) + sent[c].astype(jnp.float32)))
            normed.append(row_norm(resid[c], feedforward_norm_gain))
        away = [swap(n) for n in normed]
        hidden_away = [hidden_of(n) for n in away]
        hidden_own = hidden_of(jnp.concatenate(normed))
        hidden_away, hidden_own, down_full = lax.optimization_barrier(
            (hidden_away, hidden_own, down_full))
        partial = [down_of(h) for h in hidden_away]
        partial, hidden_own = lax.optimization_barrier((partial, hidden_own))
        returned = [swap(p) for p in partial]
        kept = down_of(hidden_own)
        return jnp.concatenate([
            (resid[c] + (kept[c * step : (c + 1) * step].astype(jnp.float32)
                         + returned[c].astype(jnp.float32))).astype(jnp.bfloat16)
            for c in range(chunks)])
    down_full = gather(down_weight, 1)
    scatter = lambda x: lax.psum_scatter(x, "tp", scatter_dimension=0, tiled=True)
    attended = scatter(product(mixed, output_weight).astype(jnp.bfloat16)).astype(jnp.float32)
    resid = own_stream + attended
    normed = lax.all_gather(row_norm(resid, feedforward_norm_gain), "tp", axis=0, tiled=True)
    mlp_out = scatter(down_of(hidden_of(normed))).astype(jnp.float32)
    return (resid + mlp_out).astype(jnp.bfloat16)


def solution(mesh):
    placed = (
        P("sp", None),
        P("sp", "tp"),
        P("sp", "tp"),
        P("sp", "tp"),
        P("sp", "tp"),
        P("tp"),
        P("sp", "tp"),
        P("sp"),
        P("sp", "tp"),
        P(),
        P("tp", None),
        P(),
        P("sp", "tp"),
        P("sp", "tp"),
        P("tp", "sp"),
    )
    return jax.shard_map(
        per_device, mesh=mesh, in_specs=placed, out_specs=P(("sp", "tp"), None), check_vma=False
    )
```
